32 devices in a mesh: rep: 2 (over x), fs: 4 (over z), tp: 4 (over y, core).
Axes of the slice: x: 2, y: 2, z: 4, core: 2. Of those that a mesh axis runs over, the one named last changes fastest.
Arguments:
- tokens: bfloat16 [8, 1024, 2048], P(('rep', 'fs')), may hold values from -6 to 6
- mix_gain: bfloat16 [2048], replicated, may hold values from 0.099609375 to 1.8984375
- value_weight: bfloat16 [2048, 1024], P('fs', 'tp'), may hold values from -0.125 to 0.125
- gate_weight: bfloat16 [2048, 1024], P('fs', 'tp'), may hold values from -0.125 to 0.125
- mix_taps: bfloat16 [31, 1024], P(None, 'tp'), may hold values from -1 to 1
- head_gain: bfloat16 [1024], P('tp'), may hold values from 0.099609375 to 1.8984375
- out_weight: bfloat16 [1024, 2048], P('fs', 'tp'), may hold values from -0.1875 to 0.1875
- ffn_gain: bfloat16 [2048], replicated, may hold values from 0.099609375 to 1.8984375
- ffgate_weight: bfloat16 [2048, 6144], P('fs', 'tp'), may hold values from -0.125 to 0.125
- up_weight: bfloat16 [2048, 6144], P('fs', 'tp'), may hold values from -0.125 to 0.125
- ff_taps: bfloat16 [3, 6144], P(None, 'tp'), may hold values from -3.5 to 3.5
- down_weight: bfloat16 [2048, 6144], P('fs', 'tp'), may hold values from -0.078125 to 0.078125
Outputs:
- layer_out: bfloat16 [8, 1024, 2048], P(('rep', 'fs'), 'tp')
The draws below stay inside these ranges and needn't reach their ends.
All inputs are finite; a program needn't handle non-finite values.
Results may differ from the reference program's by a relative error of at most 0.01.
Values may be sent and summed in bfloat16 or wider, within the bound.
A program may use at most 128 MiB of HBM per device.

```python
import jax
import jax.numpy as jnp
from jax import lax

D = 2048
CW = 1024
FF = 6144
HEAD = 128
KW = 31
KF = 3
LEN = 1024
BATCH = 8


def steps_of(stream_key, shape, cuts, smallest, largest):
    level = 1.0
    for dim, parts in cuts:
        draws = jax.random.uniform(jax.random.fold_in(jax.random.fold_in(stream_key, 6), dim), (parts,), jnp.float32, smallest / len(cuts), largest / len(cuts))
        level = level * jnp.repeat(jnp.exp(draws), shape[dim] // parts).reshape((-1,) + (1,) * (len(shape) - 1 - dim))
    return level


def normal_values(stream_key, shape, scale, bound, pieces=(), kind=jnp.bfloat16):
    level = steps_of(stream_key, shape, pieces, -0.22, 0.18) if pieces else 1.0
    array = jax.random.normal(stream_key, shape, jnp.float32) * scale * level
    return jnp.minimum(jnp.maximum(array, -bound), bound).astype(kind)


def setup_inputs(seed: int = 0) -> dict:
    key_of = jax.random.split(jax.random.key(seed), 13)
    tokens = normal_values(key_of[0], (BATCH, LEN, D), 1.0, 6.0, ((0, 8),))
    mix_gain = jnp.clip(1.0 + 0.18 * jax.random.normal(key_of[1], (D,), jnp.float32), 0.099609375, 1.8984375).astype(jnp.bfloat16)
    value_weight = normal_values(key_of[2], (D, CW), D ** -0.5, 0.125, ((0, 4), (1, 4)))
    gate_weight = normal_values(key_of[3], (D, CW), D ** -0.5, 0.125, ((0, 4), (1, 4)))
    mix_taps = normal_values(key_of[4], (KW, CW), KW ** -0.5, 1.0, ((1, 4),))
    head_gain = jnp.clip(1.0 + 0.18 * jax.random.normal(key_of[5], (CW,), jnp.float32), 0.099609375, 1.8984375).astype(jnp.bfloat16)
    out_weight = normal_values(key_of[6], (CW, D), CW ** -0.5, 0.1875, ((0, 4), (1, 4)))
    ffn_gain = jnp.clip(1.0 + 0.18 * jax.random.normal(key_of[7], (D,), jnp.float32), 0.099609375, 1.8984375).astype(jnp.bfloat16)
    ffgate_weight = normal_values(key_of[8], (D, FF), D ** -0.5, 0.125, ((0, 4), (1, 4)))
    up_weight = normal_values(key_of[9], (D, FF), D ** -0.5, 0.125, ((0, 4), (1, 4)))
    ff_taps = normal_values(key_of[10], (KF, FF), KF ** -0.5, 3.5, ((1, 4),))
    down_weight = normal_values(key_of[11], (D, FF), FF ** -0.5, 0.078125, ((0, 4), (1, 4)))
    return {"tokens": tokens, "mix_gain": mix_gain, "value_weight": value_weight, "gate_weight": gate_weight, "mix_taps": mix_taps, "head_gain": head_gain, "out_weight": out_weight, "ffn_gain": ffn_gain, "ffgate_weight": ffgate_weight, "up_weight": up_weight, "ff_taps": ff_taps, "down_weight": down_weight}


norm_floor = 0.01

def row_norm(floats_in, scales):
    floats = floats_in.astype(jnp.float32)
    scaled = floats * lax.rsqrt(lax.optimization_barrier(jnp.mean(floats * floats, axis=-1, keepdims=True)) + norm_floor)
    return (scaled * scales.astype(jnp.float32)).astype(jnp.bfloat16)

def causal_conv(signal, kernel_taps):
    reach = kernel_taps.shape[0]
    length = signal.shape[0]
    padded = jnp.pad(signal, ((reach - 1, 0), (0, 0)))
    summed = padded[0:length] * kernel_taps[0]
    for offset in range(1, reach):
        summed = summed + padded[offset:offset + length] * kernel_taps[offset]
    return summed

def head_norm(signal, scales):
    length = signal.shape[0]
    grouped = signal.reshape(length, signal.shape[1] // HEAD, HEAD)
    centre = grouped - lax.optimization_barrier(jnp.mean(grouped, axis=-1, keepdims=True))
    spread = lax.optimization_barrier(jnp.mean(centre * centre, axis=-1, keepdims=True))
    normal = (centre * lax.rsqrt(spread + norm_floor)).reshape(signal.shape)
    return normal * scales.astype(jnp.float32)

def reference(tokens, mix_gain, value_weight, gate_weight, mix_taps, head_gain, out_weight, ffn_gain, ffgate_weight, up_weight, ff_taps, down_weight):

    def sublayers(sequence):
        normed = row_norm(sequence, mix_gain)
        values = jnp.dot(normed, value_weight, preferred_element_type=jnp.float32)
        gating = jnp.dot(normed, gate_weight, preferred_element_type=jnp.float32)
        glu_out = values * jax.nn.sigmoid(gating)
        mixed_pos = causal_conv(glu_out, mix_taps.astype(jnp.float32))
        head_out = jax.nn.silu(head_norm(mixed_pos, head_gain)).astype(jnp.bfloat16)
        hidden = (sequence.astype(jnp.float32) + jnp.dot(head_out, out_weight, preferred_element_type=jnp.float32)).astype(jnp.bfloat16)
        normed_ffn = row_norm(hidden, ffn_gain)
        ffgate = jnp.dot(normed_ffn, ffgate_weight, preferred_element_type=jnp.float32)
        ff_up = jnp.dot(normed_ffn, up_weight, preferred_element_type=jnp.float32)
        product = (jax.nn.silu(causal_conv(ffgate, ff_taps.astype(jnp.float32))) * ff_up).astype(jnp.bfloat16)
        down_sum = lax.dot_general(product, down_weight, (((1,), (1,)), ((), ())), preferred_element_type=jnp.float32)
        return (hidden.astype(jnp.float32) + down_sum).astype(jnp.bfloat16)
    return lax.map(sublayers, tokens)
```

```python
import functools

import jax
import jax.numpy as jnp
from jax import lax
from jax.experimental import pallas as pl
from jax.experimental.pallas import tpu as pltpu
from jax.sharding import PartitionSpec as P

HEAD = 128
MESH = pl.DeviceIdType.MESH
F32 = jnp.float32
BF16 = jnp.bfloat16
norm_floor = 0.01


def row_norm(floats_in, scales):
    floats = floats_in.astype(F32)
    scaled = floats * lax.rsqrt(jnp.mean(floats * floats, axis=-1, keepdims=True) + norm_floor)
    return (scaled * scales.astype(F32)).astype(BF16)


def causal_conv(signal, kernel_taps):
    reach = kernel_taps.shape[0]
    length = signal.shape[0]
    padded = jnp.pad(signal, ((reach - 1, 0), (0, 0)))
    summed = padded[0:length] * kernel_taps[0]
    for offset in range(1, reach):
        summed = summed + padded[offset : offset + length] * kernel_taps[offset]
    return summed


def head_norm(signal, scales):
    heads = []
    for start in range(0, signal.shape[1], HEAD):
        part = signal[:, start : start + HEAD]
        centre = part - jnp.mean(part, axis=-1, keepdims=True)
        spread = jnp.mean(centre * centre, axis=-1, keepdims=True)
        gain = scales[start : start + HEAD].astype(F32)
        heads.append(jax.nn.silu(centre * lax.rsqrt(spread + norm_floor) * gain))
    return jnp.concatenate(heads, axis=1).astype(BF16)


def plain(
    tokens,
    mix_gain,
    value_weight,
    gate_weight,
    mix_taps,
    head_gain,
    out_weight,
    ffn_gain,
    ffgate_weight,
    up_weight,
    ff_taps,
    down_weight,
):
    def rows_of(shard):
        return lax.all_gather(shard, "fs", axis=0, tiled=True)

    sequence = tokens[0]
    width = value_weight.shape[1]
    pair_full = rows_of(jnp.concatenate([value_weight, gate_weight], axis=1))
    out_full = rows_of(out_weight)
    normed = row_norm(sequence, mix_gain)
    both = jnp.dot(normed, pair_full, preferred_element_type=F32)
    glu_out = both[:, :width] * jax.nn.sigmoid(both[:, width:])
    mixed_pos = causal_conv(glu_out, mix_taps.astype(F32))
    head_out = head_norm(mixed_pos, head_gain)
    out_cols = out_full.shape[1]
    all_heads = lax.all_gather(head_out, "tp", axis=1, tiled=True)
    own_cols = lax.dynamic_slice_in_dim(sequence, lax.axis_index("tp") * out_cols, out_cols, 1)
    mixer_sum = jnp.dot(all_heads, out_full, preferred_element_type=F32)
    hidden_cols = (own_cols.astype(F32) + mixer_sum).astype(BF16)
    full_rows = lax.all_gather(hidden_cols, "tp", axis=1, tiled=True)
    normed_ffn = row_norm(full_rows, ffn_gain)
    ffgate = jnp.dot(normed_ffn, rows_of(ffgate_weight), preferred_element_type=F32)
    gated = jax.nn.silu(causal_conv(ffgate, ff_taps.astype(F32)))
    ff_up = jnp.dot(normed_ffn, rows_of(up_weight), preferred_element_type=F32)
    product = (gated * ff_up).astype(BF16)
    own_count = sequence.shape[0] // lax.axis_size("tp")
    own_rows = lax.dynamic_slice_in_dim(full_rows, lax.axis_index("tp") * own_count, own_count, 0)
    partial = lax.dot_general(
        product, rows_of(down_weight), (((1,), (1,)), ((), ())), preferred_element_type=F32
    )
    result = lax.psum_scatter(partial.astype(BF16), "tp", scatter_dimension=0, tiled=True)
    return (own_rows.astype(F32) + result.astype(F32)).astype(BF16)[None]


def kernel(
    tokens,
    mix_gain,
    value_w,
    gate_w,
    mix_taps,
    head_gain,
    out_w,
    ffn_gain,
    ffgate_w,
    up_w,
    ff_taps,
    down_w,
    out,
    tok,
    normed,
    wpair,
    wout,
    glu,
    heads,
    hid,
    xc,
    wg,
    wu,
    wd,
    gbuf,
    ubuf,
    prod,
    part,
    rs1,
    sum1,
    rs2,
    sum2,
    rs3,
    loc,
    tsem,
    zs,
    zr,
    xs,
    xr,
    hs,
    hr,
    es,
    er,
    qs,
    qr,
):
    r, f, t = lax.axis_index("rep"), lax.axis_index("fs"), lax.axis_index("tp")
    y, c = t // 2, t % 2
    zl, zh = f % 2, f // 2
    fp = f + 1 - 2 * zl
    sib, ynb = t + 1 - 2 * c, (t + 2) % 4
    far = (sib + 2) % 4
    to_x, to_z, to_sib, to_y = {"rep": 1 - r}, {"fs": fp}, {"tp": sib}, {"tp": ynb}

    length, width = tok.shape
    chunk = length // 4
    cw = value_w.shape[1]
    ow = out_w.shape[1]
    hw = wg.shape[1]
    feat = down_w.shape[0] // 2

    def remote(src, dst, ss, rs, where):
        return pltpu.make_async_remote_copy(
            src_ref=src, dst_ref=dst, send_sem=ss, recv_sem=rs, device_id=where, device_id_type=MESH
        )

    barrier = pltpu.get_barrier_semaphore()
    for peer in (to_x, to_sib, to_y, {"fs": (f + 1) % 4}, {"fs": (f + 2) % 4}, {"fs": (f + 3) % 4}):
        pl.semaphore_signal(barrier, inc=1, device_id=peer, device_id_type=MESH)

    def rows(j):
        return pl.ds(pl.multiple_of(j * chunk, chunk), chunk)

    def tok_copy(j):
        return pltpu.make_async_copy(tokens.at[0, rows(j), :], tok.at[rows(j), :], tsem.at[j])

    for j in range(4):
        tok_copy(j).start()

    mats = (
        (value_w, wpair, 0, False),
        (gate_w, wpair, cw, False),
        (out_w, wout, 0, False),
        (ffgate_w, wg, 0, True),
        (up_w, wu, 0, True),
        (down_w, wd, 0, True),
    )

    def src_of(m, row, count, parity):
        w, dst, col, halves = mats[m]
        if halves:
            return w.at[pl.ds(row, count), pl.ds(pl.multiple_of(parity * hw, 128), hw)]
        return w.at[pl.ds(row, count), :]

    def dst_of(m, row, count):
        w, dst, col, halves = mats[m]
        size = hw if halves else w.shape[1]
        return dst.at[pl.ds(row, count), pl.ds(col, size)]

    def piece(m, owner, half):
        n = mats[m][0].shape[0]
        return dst_of(m, pl.multiple_of(owner * n + half * (n // 2), n // 2), n // 2)

    def own_copy(m):
        n = mats[m][0].shape[0]
        return pltpu.make_async_copy(
            src_of(m, 0, n, zl), dst_of(m, pl.multiple_of(f * n, n), n), loc.at[m]
        )

    def z_copy(m, target):
        n = mats[m][0].shape[0]
        return remote(
            src_of(m, pl.multiple_of(r * (n // 2), n // 2), n // 2, target % 2),
            piece(m, f, r),
            zs.at[m, target],
            zr.at[m, f],
            {"fs": target},
        )

    def z_arrived(m, owner):
        n = mats[m][0].shape[0]
        remote(piece(m, owner, r), piece(m, owner, r), zs.at[m, owner], zr.at[m, owner], to_x).wait_recv()

    def x_copy(m, owner):
        return remote(piece(m, owner, r), piece(m, owner, r), xs.at[m, owner], xr.at[m, owner], to_x)

    def x_arrived(m, owner):
        remote(
            piece(m, owner, 1 - r), piece(m, owner, 1 - r), xs.at[m, owner], xr.at[m, owner], to_x
        ).wait_recv()

    def others(fn):
        def step(k, carry):
            fn((f + k) % 4)
            return carry

        lax.fori_loop(1, 4, step, 0)

    for m in range(6):
        own_copy(m).start()
    pl.semaphore_wait(barrier, 6)

    def send_weights(*ms):
        def one(target):
            for m in ms:
                z_copy(m, target).start()

        others(one)

    def pass_on(*ms):
        def one(owner):
            for m in ms:
                z_arrived(m, owner)
                x_copy(m, owner).start()

        others(one)

    def collect(*ms):
        def one(owner):
            for m in ms:
                x_arrived(m, owner)

        others(one)
        for m in ms:
            own_copy(m).wait()

    send_weights(0, 1)
    send_weights(2)
    send_weights(3)

    def norm_rows(src, dst, gain_ref, count):
        gain = gain_ref[...].astype(F32)

        def step(i, carry):
            at = pl.ds(pl.multiple_of(i * 16, 16), 16)
            v = src[at, :].astype(F32)
            s = lax.rsqrt(jnp.mean(v * v, axis=-1, keepdims=True) + norm_floor)
            dst[at, :] = (v * s * gain).astype(BF16)
            return carry

        lax.fori_loop(0, count // 16, step, 0, unroll=4)

    glu[pl.ds(0, 32), :] = jnp.zeros((32, cw), F32)
    for j in range(4):
        tok_copy(j).wait()
    norm_rows(tok, normed, mix_gain, length)

    pass_on(0, 1)
    collect(0, 1)

    def head_cols(who):
        return pl.ds(pl.multiple_of(who * cw, 128), cw)

    def head_send(kind, j, who, where):
        block = heads.at[rows(j), head_cols(who)]
        return remote(block, block, hs.at[kind, j], hr.at[kind, j], where)

    def head_wait(kind, j, who):
        block = heads.at[rows(j), head_cols(who)]
        remote(block, block, hs.at[kind, j], hr.at[kind, j], to_sib).wait_recv()

    reach = mix_taps.shape[0]
    sub = 32

    def mix_chunk(j, carry):
        both = jnp.dot(normed[rows(j), :], wpair[...], preferred_element_type=F32)
        glu[pl.ds(pl.multiple_of(j * chunk + 32, 32), chunk), :] = both[:, :cw] * jax.nn.sigmoid(both[:, cw:])

        def conv_step(i, inner):
            base = pl.multiple_of(j * chunk + i * sub, sub)
            window = glu[pl.ds(base, sub + 32), :]
            acc = None
            for k in range(reach):
                o = 32 - (reach - 1) + k
                term = window[o : o + sub, :] * mix_taps[k : k + 1, :].astype(F32)
                acc = term if acc is None else acc + term
            parts = []
            for h in range(0, cw, HEAD):
                v = acc[:, h : h + HEAD]
                v = v - jnp.mean(v, axis=-1, keepdims=True)
                s = lax.rsqrt(jnp.mean(v * v, axis=-1, keepdims=True) + norm_floor)
                v = v * s * head_gain[:, h : h + HEAD].astype(F32)
                parts.append(v * jax.nn.sigmoid(v))
            heads[pl.ds(base, sub), head_cols(t)] = jnp.concatenate(parts, axis=1).astype(BF16)
            return inner

        lax.fori_loop(0, chunk // sub, conv_step, 0)
        head_send(0, j, t, to_sib).start()
        head_send(1, j, t, to_y).start()
        return carry

    lax.fori_loop(0, 4, mix_chunk, 0)
    pass_on(2)

    def heads_on(j, carry):
        head_wait(1, j, ynb)
        head_send(2, j, ynb, to_sib).start()
        return carry

    lax.fori_loop(0, 4, heads_on, 0)
    collect(2)

    def hid_block(seq, j, who):
        return hid.at[seq, rows(j), pl.ds(pl.multiple_of(who * ow, 128), ow)]

    def hid_send(kind, j, seq, who, where):
        block = hid_block(seq, j, who)
        return remote(block, block, es.at[kind, j], er.at[kind, j], where)

    def hid_wait(kind, j, seq, who):
        block = hid_block(seq, j, who)
        remote(block, block, es.at[kind, j], er.at[kind, j], to_sib).wait_recv()

    def out_chunk(j, carry):
        head_wait(0, j, sib)
        head_wait(2, j, far)
        own = tok[rows(j), pl.ds(pl.multiple_of(t * ow, 128), ow)].astype(F32)
        total = own + jnp.dot(heads[rows(j), :], wout[...], preferred_element_type=F32)
        hid[zl, rows(j), pl.ds(pl.multiple_of(t * ow, 128), ow)] = total.astype(BF16)
        hid_send(0, j, zl, t, to_sib).start()
        hid_send(1, j, zl, t, to_y).start()
        hid_send(2, j, zl, t, to_z).start()
        return carry

    lax.fori_loop(0, 4, out_chunk, 0)
    send_weights(4)
    send_weights(5)

    def hid_on(j, carry):
        hid_wait(1, j, zl, ynb)
        hid_send(3, j, zl, ynb, to_sib).start()
        hid_wait(2, j, 1 - zl, t)
        hid_send(4, j, 1 - zl, t, to_sib).start()
        hid_send(5, j, 1 - zl, t, to_y).start()
        return carry

    lax.fori_loop(0, 4, hid_on, 0)
    pass_on(3)

    def hid_on2(j, carry):
        hid_wait(5, j, 1 - zl, ynb)
        hid_send(6, j, 1 - zl, ynb, to_sib).start()
        return carry

    lax.fori_loop(0, 4, hid_on2, 0)
    pass_on(4)
    collect(3, 4)

    freach = ff_taps.shape[0]
    asub = 32

    def ffn_chunk(i, carry):
        first = i < 4
        j = i % 4
        seq = jnp.where(first, zl, 1 - zl)

        @pl.when(first)
        def _():
            hid_wait(0, j, zl, sib)
            hid_wait(3, j, zl, far)

        @pl.when(jnp.logical_not(first))
        def _():
            hid_wait(4, j, 1 - zl, sib)
            hid_wait(6, j, 1 - zl, far)

        norm_rows(hid.at[seq, rows(j), :], xc, ffn_gain, chunk)
        keep = jnp.where(j == 0, 0.0, 1.0)
        gbuf[pl.ds(0, 8), :] = gbuf[pl.ds(chunk, 8), :]

        @pl.when(j == 0)
        def _():
            gbuf[pl.ds(0, 8), :] = jnp.zeros((8, hw), F32)

        gbuf[pl.ds(8, chunk), :] = jnp.dot(xc[...], wg[...], preferred_element_type=F32)
        ubuf[...] = jnp.dot(xc[...], wu[...], preferred_element_type=F32)

        def act(a, inner):
            base = pl.multiple_of(a * asub, asub)
            window = gbuf[pl.ds(base, asub + 8), :]
            acc = None
            for k in range(freach):
                o = 8 - (freach - 1) + k
                term = window[o : o + asub, :] * ff_taps[k : k + 1, :].astype(F32)
                acc = term if acc is None else acc + term
            v = acc * jax.nn.sigmoid(acc) * ubuf[pl.ds(base, asub), :]
            prod[pl.ds(pl.multiple_of(seq * length + j * chunk + base, asub), asub), :] = v.astype(BF16)
            return inner

        lax.fori_loop(0, chunk // asub, act, 0)
        return carry

    lax.fori_loop(0, 8, ffn_chunk, 0)

    own_copy(5).wait()
    blocks = 8

    def place(i):
        late = i // 4
        k = i % 4
        owner = jnp.where(late == 0, 2 * zh + k // 2, 2 * (1 - zh) + k % 2)
        flip = jnp.where(late == 0, k % 2, k // 2)
        half = jnp.where(flip == 0, r, 1 - r)
        return owner, flip, half

    def q1(i):
        return remote(part.at[i % 3, 1 - c], rs1.at[i], qs.at[0, i], qr.at[0, i], to_sib)

    def q2(i):
        return remote(sum1.at[i % 3, 1 - y], rs2.at[i], qs.at[1, i], qr.at[1, i], to_y)

    def q3(i):
        return remote(sum2.at[i % 3, 1 - zl], rs3.at[i], qs.at[2, i], qr.at[2, i], to_z)

    def turn(i, carry):
        @pl.when(i == 0)
        def _():
            z_arrived(5, fp)
            x_copy(5, fp).start()

        @pl.when((i == 2) | (i == 3))
        def _():
            owner = 2 * (1 - zh) + i % 2
            z_arrived(5, owner)
            x_copy(5, owner).start()

        @pl.when(i < blocks)
        def _():
            owner, flip, half = place(i)

            @pl.when((owner != f) & (flip == 1))
            def _():
                x_arrived(5, owner)

            @pl.when(i >= 3)
            def _():
                q1(i - 3).wait_send()

            at = pl.ds(pl.multiple_of(owner * 2 * feat + half * feat, feat), feat)

            def block_rows(b, inner):
                cc, yy, ss = b // 4, (b // 2) % 2, b % 2
                row = pl.multiple_of(ss * length + (2 * yy + cc) * chunk, chunk)
                part[i % 3, cc, yy, ss] = lax.dot_general(
                    prod[pl.ds(row, chunk), :],
                    wd[at, :],
                    (((1,), (1,)), ((), ())),
                    preferred_element_type=F32,
                ).astype(BF16)
                return inner

            lax.fori_loop(0, 8, block_rows, 0)
            q1(i).start()

        @pl.when((i >= 1) & (i <= blocks))
        def _():
            n = i - 1
            q1(n).wait_recv()

            @pl.when(n >= 3)
            def _():
                q2(n - 3).wait_send()

            sum1[n % 3] = (part[n % 3, c].astype(F32) + rs1[n].astype(F32)).astype(BF16)
            q2(n).start()

        @pl.when((i >= 2) & (i <= blocks + 1))
        def _():
            n = i - 2
            q2(n).wait_recv()

            @pl.when(n >= 3)
            def _():
                q3(n - 3).wait_send()

            sum2[n % 3] = (sum1[n % 3, y].astype(F32) + rs2[n].astype(F32)).astype(BF16)
            q3(n).start()

        @pl.when(i >= 3)
        def _():
            n = i - 3
            q3(n).wait_recv()
            owner, flip, half = place(n)
            cols = pl.ds(pl.multiple_of(owner * 2 * feat + half * feat, feat), feat)
            base = hid[zl, pl.ds(pl.multiple_of(t * chunk, chunk), chunk), cols].astype(F32)
            total = base + (sum2[n % 3, zl].astype(F32) + rs3[n].astype(F32))
            out[0, :, cols] = total.astype(BF16)

        return carry

    lax.fori_loop(0, blocks + 3, turn, 0)

    for n in range(blocks - 3, blocks):
        q1(n).wait_send()
        q2(n).wait_send()
        q3(n).wait_send()

    def drain(target):
        for m in range(6):
            z_copy(m, target).wait_send()
            x_copy(m, target).wait_send()

    others(drain)

    def drain_chunks(j, carry):
        head_send(0, j, t, to_sib).wait_send()
        head_send(1, j, t, to_y).wait_send()
        head_send(2, j, ynb, to_sib).wait_send()
        hid_send(0, j, zl, t, to_sib).wait_send()
        hid_send(1, j, zl, t, to_y).wait_send()
        hid_send(2, j, zl, t, to_z).wait_send()
        hid_send(3, j, zl, ynb, to_sib).wait_send()
        hid_send(4, j, 1 - zl, t, to_sib).wait_send()
        hid_send(5, j, 1 - zl, t, to_y).wait_send()
        hid_send(6, j, 1 - zl, ynb, to_sib).wait_send()
        return carry

    lax.fori_loop(0, 4, drain_chunks, 0)


def fused(*arrays):
    (tokens, mix_gain, value_w, gate_w, mix_taps, head_gain, out_w, ffn_gain, ffgate_w, up_w, ff_taps, down_w) = arrays
    _, length, width = tokens.shape
    fs = lax.axis_size("fs")
    cw, ow = value_w.shape[1], out_w.shape[1]
    hw = ffgate_w.shape[1] // 2
    chunk = length // 4
    feat = down_w.shape[0] // 2
    zl = lax.axis_index("fs") % 2
    taps = lax.dynamic_slice_in_dim(ff_taps, zl * hw, hw, 1)
    scratch = [
        pltpu.VMEM((length, width), BF16),
        pltpu.VMEM((length, width), BF16),
        pltpu.VMEM((fs * value_w.shape[0], 2 * cw), BF16),
        pltpu.VMEM((fs * out_w.shape[0], ow), BF16),
        pltpu.VMEM((length + 32, cw), F32),
        pltpu.VMEM((length, 4 * cw), BF16),
        pltpu.VMEM((2, length, width), BF16),
        pltpu.VMEM((chunk, width), BF16),
        pltpu.VMEM((fs * ffgate_w.shape[0], hw), BF16),
        pltpu.VMEM((fs * up_w.shape[0], hw), BF16),
        pltpu.VMEM((fs * down_w.shape[0], hw), BF16),
        pltpu.VMEM((chunk + 8, hw), F32),
        pltpu.VMEM((chunk, hw), F32),
        pltpu.VMEM((2 * length, hw), BF16),
        pltpu.VMEM((3, 2, 2, 2, chunk, feat), BF16),
        pltpu.VMEM((8, 2, 2, chunk, feat), BF16),
        pltpu.VMEM((3, 2, 2, chunk, feat), BF16),
        pltpu.VMEM((8, 2, chunk, feat), BF16),
        pltpu.VMEM((3, 2, chunk, feat), BF16),
        pltpu.VMEM((8, chunk, feat), BF16),
        pltpu.SemaphoreType.DMA((6,)),
        pltpu.SemaphoreType.DMA((4,)),
    ]
    scratch += [pltpu.SemaphoreType.DMA((6, 4))] * 4
    scratch += [pltpu.SemaphoreType.DMA((3, 4))] * 2
    scratch += [pltpu.SemaphoreType.DMA((7, 4))] * 2
    scratch += [pltpu.SemaphoreType.DMA((3, 8))] * 2
    anywhere = pl.BlockSpec(memory_space=pl.ANY)
    small = pl.BlockSpec(memory_space=pltpu.VMEM)
    return pl.pallas_call(
        kernel,
        out_shape=jax.ShapeDtypeStruct((1, chunk, width), BF16),
        in_specs=[anywhere, small, anywhere, anywhere, small, small, anywhere, small, anywhere, anywhere, small, anywhere],
        out_specs=small,
        scratch_shapes=scratch,
        compiler_params=pltpu.CompilerParams(
            collective_id=0, has_side_effects=True, vmem_limit_bytes=67043328
        ),
        name="layer",
    )(
        tokens,
        mix_gain[None],
        value_w,
        gate_w,
        mix_taps,
        head_gain[None],
        out_w,
        ffn_gain[None],
        ffgate_w,
        up_w,
        taps,
        down_w,
    )


def solution(mesh):
    placed = (
        P(("rep", "fs"), None, None),
        P(),
        P("fs", "tp"),
        P("fs", "tp"),
        P(None, "tp"),
        P("tp"),
        P("fs", "tp"),
        P(),
        P("fs", "tp"),
        P("fs", "tp"),
        P(None, "tp"),
        P("fs", "tp"),
    )
    shape = mesh.shape
    small = shape["rep"] == 2 and shape["fs"] == 4 and shape["tp"] == 4
    return jax.shard_map(
        fused if small else plain,
        mesh=mesh,
        in_specs=placed,
        out_specs=P(("rep", "fs"), "tp", None),
        check_vma=False,
    )
```

```python
import functools

import jax
import jax.numpy as jnp
from jax import lax
from jax.experimental import pallas as pl
from jax.experimental.pallas import tpu as pltpu
from jax.sharding import PartitionSpec as P

HEAD = 128
MESH = pl.DeviceIdType.MESH
F32 = jnp.float32
BF16 = jnp.bfloat16
norm_floor = 0.01


def row_norm(floats_in, scales):
    floats = floats_in.astype(F32)
    scaled = floats * lax.rsqrt(jnp.mean(floats * floats, axis=-1, keepdims=True) + norm_floor)
    return (scaled * scales.astype(F32)).astype(BF16)


def causal_conv(signal, kernel_taps):
    reach = kernel_taps.shape[0]
    length = signal.shape[0]
    padded = jnp.pad(signal, ((reach - 1, 0), (0, 0)))
    summed = padded[0:length] * kernel_taps[0]
    for offset in range(1, reach):
        summed = summed + padded[offset : offset + length] * kernel_taps[offset]
    return summed


def head_norm(signal, scales):
    heads = []
    for start in range(0, signal.shape[1], HEAD):
        part = signal[:, start : start + HEAD]
        centre = part - jnp.mean(part, axis=-1, keepdims=True)
        spread = jnp.mean(centre * centre, axis=-1, keepdims=True)
        gain = scales[start : start + HEAD].astype(F32)
        heads.append(jax.nn.silu(centre * lax.rsqrt(spread + norm_floor) * gain))
    return jnp.concatenate(heads, axis=1).astype(BF16)


def plain(
    tokens,
    mix_gain,
    value_weight,
    gate_weight,
    mix_taps,
    head_gain,
    out_weight,
    ffn_gain,
    ffgate_weight,
    up_weight,
    ff_taps,
    down_weight,
):
    def rows_of(shard):
        return lax.all_gather(shard, "fs", axis=0, tiled=True)

    sequence = tokens[0]
    width = value_weight.shape[1]
    pair_full = rows_of(jnp.concatenate([value_weight, gate_weight], axis=1))
    out_full = rows_of(out_weight)
    normed = row_norm(sequence, mix_gain)
    both = jnp.dot(normed, pair_full, preferred_element_type=F32)
    glu_out = both[:, :width] * jax.nn.sigmoid(both[:, width:])
    mixed_pos = causal_conv(glu_out, mix_taps.astype(F32))
    head_out = head_norm(mixed_pos, head_gain)
    out_cols = out_full.shape[1]
    all_heads = lax.all_gather(head_out, "tp", axis=1, tiled=True)
    own_cols = lax.dynamic_slice_in_dim(sequence, lax.axis_index("tp") * out_cols, out_cols, 1)
    mixer_sum = jnp.dot(all_heads, out_full, preferred_element_type=F32)
    hidden_cols = (own_cols.astype(F32) + mixer_sum).astype(BF16)
    full_rows = lax.all_gather(hidden_cols, "tp", axis=1, tiled=True)
    normed_ffn = row_norm(full_rows, ffn_gain)
    ffgate = jnp.dot(normed_ffn, rows_of(ffgate_weight), preferred_element_type=F32)
    gated = jax.nn.silu(causal_conv(ffgate, ff_taps.astype(F32)))
    ff_up = jnp.dot(normed_ffn, rows_of(up_weight), preferred_element_type=F32)
    product = (gated * ff_up).astype(BF16)
    own_count = sequence.shape[0] // lax.axis_size("tp")
    own_rows = lax.dynamic_slice_in_dim(full_rows, lax.axis_index("tp") * own_count, own_count, 0)
    partial = lax.dot_general(
        product, rows_of(down_weight), (((1,), (1,)), ((), ())), preferred_element_type=F32
    )
    result = lax.psum_scatter(partial.astype(BF16), "tp", scatter_dimension=0, tiled=True)
    return (own_rows.astype(F32) + result.astype(F32)).astype(BF16)[None]


def kernel(
    tokens,
    mix_gain,
    value_w,
    gate_w,
    mix_taps,
    head_gain,
    out_w,
    ffn_gain,
    ffgate_w,
    up_w,
    ff_taps,
    down_w,
    out,
    tok,
    normed,
    wpair,
    wout,
    glu,
    heads,
    hid,
    xc,
    tapb,
    wg,
    wu,
    wd,
    gbuf,
    ubuf,
    prod,
    part,
    rs1,
    sum1,
    rs2,
    sum2,
    rs3,
    loc,
    tsem,
    zs,
    zr,
    xs,
    xr,
    hs,
    hr,
    es,
    er,
    qs,
    qr,
):
    r, f, t = lax.axis_index("rep"), lax.axis_index("fs"), lax.axis_index("tp")
    y, c = t // 2, t % 2
    zl, zh = f % 2, f // 2
    fp = f + 1 - 2 * zl
    sib, ynb = t + 1 - 2 * c, (t + 2) % 4
    far = (sib + 2) % 4
    to_x, to_z, to_sib, to_y = {"rep": 1 - r}, {"fs": fp}, {"tp": sib}, {"tp": ynb}

    length, width = tok.shape
    chunk = length // 4
    cw = value_w.shape[1]
    ow = out_w.shape[1]
    hw = wg.shape[1]
    feat = down_w.shape[0] // 2

    def remote(src, dst, ss, rs, where):
        return pltpu.make_async_remote_copy(
            src_ref=src, dst_ref=dst, send_sem=ss, recv_sem=rs, device_id=where, device_id_type=MESH
        )

    barrier = pltpu.get_barrier_semaphore()
    for peer in (to_x, to_sib, to_y, {"fs": (f + 1) % 4}, {"fs": (f + 2) % 4}, {"fs": (f + 3) % 4}):
        pl.semaphore_signal(barrier, inc=1, device_id=peer, device_id_type=MESH)

    def rows(j):
        return pl.ds(pl.multiple_of(j * chunk, chunk), chunk)

    def tok_copy(j):
        return pltpu.make_async_copy(tokens.at[0, rows(j), :], tok.at[rows(j), :], tsem.at[j])

    for j in range(4):
        tok_copy(j).start()

    mats = (
        (value_w, wpair, 0, False),
        (gate_w, wpair, cw, False),
        (out_w, wout, 0, False),
        (ffgate_w, wg, 0, True),
        (up_w, wu, 0, True),
        (down_w, wd, 0, True),
    )

    def src_of(m, row, count, parity):
        w, dst, col, halves = mats[m]
        if halves:
            return w.at[pl.ds(row, count), pl.ds(pl.multiple_of(parity * hw, 128), hw)]
        return w.at[pl.ds(row, count), :]

    def dst_of(m, row, count):
        w, dst, col, halves = mats[m]
        size = hw if halves else w.shape[1]
        return dst.at[pl.ds(row, count), pl.ds(col, size)]

    def piece(m, owner, half):
        n = mats[m][0].shape[0]
        return dst_of(m, pl.multiple_of(owner * n + half * (n // 2), n // 2), n // 2)

    def own_copy(m):
        n = mats[m][0].shape[0]
        return pltpu.make_async_copy(
            src_of(m, 0, n, zl), dst_of(m, pl.multiple_of(f * n, n), n), loc.at[m]
        )

    def z_copy(m, target):
        n = mats[m][0].shape[0]
        return remote(
            src_of(m, pl.multiple_of(r * (n // 2), n // 2), n // 2, target % 2),
            piece(m, f, r),
            zs.at[m, target],
            zr.at[m, f],
            {"fs": target},
        )

    def z_arrived(m, owner):
        n = mats[m][0].shape[0]
        remote(piece(m, owner, r), piece(m, owner, r), zs.at[m, owner], zr.at[m, owner], to_x).wait_recv()

    def x_copy(m, owner):
        return remote(piece(m, owner, r), piece(m, owner, r), xs.at[m, owner], xr.at[m, owner], to_x)

    def x_arrived(m, owner):
        remote(
            piece(m, owner, 1 - r), piece(m, owner, 1 - r), xs.at[m, owner], xr.at[m, owner], to_x
        ).wait_recv()

    def others(fn):
        def step(k, carry):
            fn(jnp.where(k == 0, fp, jnp.where(k == 1, 2 - zh, 3 - 3 * zh)))
            return carry

        lax.fori_loop(0, 3, step, 0)

    order = (fp, 2 - zh, 3 - 3 * zh)

    def line_copy(m, owner, target, slot, own):
        n = mats[m][0].shape[0]
        if own:
            src = src_of(m, pl.multiple_of(r * (n // 2), n // 2), n // 2, 0)
        else:
            src = piece(m, owner, r)
        return remote(src, piece(m, owner, r), zs.at[m, slot], zr.at[m, owner], {"fs": target})

    def end_to_end(target):
        return (f - target) * (f - target) == 9

    def z_bulk(m, fn, keep):
        def one(target):
            ok = keep(target)
            if mats[m][3]:
                ok = ok & jnp.logical_not(end_to_end(target))

            @pl.when(ok)
            def _():
                fn(z_copy(m, target))

        others(one)

    middle = (f == 1) | (f == 2)

    def across(m):
        return remote(piece(m, fp, r), piece(m, fp, r), zs.at[m, f], zr.at[m, fp], {"fs": 3 - fp})

    for m in range(6):
        own_copy(m).start()
    with jax.named_scope("barrier"):
        pl.semaphore_wait(barrier, 6)

    def start(copy):
        copy.start()

    def send_weights(*ms, keep=lambda target: target >= 0):
        for m in ms:
            z_bulk(m, start, keep)

    def pass_on(m, *which):
        for k in which:
            owner = order[k]
            z_arrived(m, owner)
            if mats[m][3] and k == 0:

                @pl.when(middle)
                def _():
                    across(m).start()

            x_copy(m, owner).start()

    def bulk_up():
        send_weights(2, 3, 4, keep=lambda target: target > f)

    def bulk_down():
        send_weights(2, 3, 4, keep=lambda target: target < f)

    def relay(d):
        for sign in (-1, 1):
            owner = f + sign * d

            @pl.when((owner >= 0) & (owner <= 3))
            def _():
                for m in (0, 1):
                    z_arrived(m, owner)
                    after = f - sign

                    @pl.when((after >= 0) & (after <= 3))
                    def _():
                        line_copy(m, owner, after, owner, False).start()

                    x_copy(m, owner).start()

        pl.when(f == d)(bulk_up)
        pl.when(3 - f == d)(bulk_down)

    def collect(*ms):
        def one(owner):
            for m in ms:
                x_arrived(m, owner)

        others(one)
        for m in ms:
            own_copy(m).wait()

    @pl.when(f < 3)
    def _():
        for m in (0, 1):
            line_copy(m, f, f + 1, 4, True).start()

    @pl.when(f > 0)
    def _():
        for m in (0, 1):
            line_copy(m, f, f - 1, 5, True).start()

    pl.when(f == 0)(bulk_up)
    pl.when(f == 3)(bulk_down)

    def norm_rows(src, dst, gain_ref, count):
        gain = gain_ref[...].astype(F32).reshape(1, width)

        def step(i, carry):
            at = pl.ds(pl.multiple_of(i * 16, 16), 16)
            v = src[at, :].astype(F32)
            s = lax.rsqrt(jnp.mean(v * v, axis=-1, keepdims=True) + norm_floor)
            dst[at, :] = (v * s * gain).astype(BF16)
            return carry

        lax.fori_loop(0, count // 16, step, 0, unroll=4)

    glu[pl.ds(0, 32), :] = jnp.zeros((32, cw), F32)
    for k in range(mix_taps.shape[0]):
        tapb[pl.ds(8 * k, 8), :] = jnp.broadcast_to(mix_taps[k : k + 1, :].astype(F32), (8, mix_taps.shape[1]))
    with jax.named_scope("tokwait"):
        for j in range(4):
            tok_copy(j).wait()
        norm_rows(tok, normed, mix_gain, length)

    with jax.named_scope("pass01"):
        for d in (1, 2, 3):
            relay(d)
    with jax.named_scope("coll01"):
        collect(0, 1)

    def head_cols(who):
        return pl.ds(pl.multiple_of(who * cw, 128), cw)

    def head_send(kind, j, who, where):
        block = heads.at[rows(j), head_cols(who)]
        return remote(block, block, hs.at[kind, j], hr.at[kind, j], where)

    def head_wait(kind, j, who):
        block = heads.at[rows(j), head_cols(who)]
        remote(block, block, hs.at[kind, j], hr.at[kind, j], to_sib).wait_recv()

    reach = mix_taps.shape[0]
    sub = 64

    hgain = head_gain[...].astype(F32).reshape(1, cw)

    def mix_chunk(j, carry):
        both = jnp.dot(normed[rows(j), :], wpair[...], preferred_element_type=F32)
        glu[pl.ds(pl.multiple_of(j * chunk + 32, 32), chunk), :] = both[:, :cw] * jax.nn.sigmoid(both[:, cw:])

        def conv_step(i, inner):
            base = pl.multiple_of(j * chunk + i * sub, sub)
            acc = None
            for e in range(8):
                rot = None
                for o in range(e, 33, 8):
                    k = o - (33 - reach)
                    if 0 <= k < reach:
                        view = glu[pl.ds(base + 8 * (o // 8), sub + 8), :].reshape(sub // 8 + 1, 8, cw)
                        term = view * tapb[pl.ds(8 * k, 8), :][None]
                        rot = term if rot is None else rot + term
                part_sum = rot.reshape(sub + 8, cw)[e : e + sub, :]
                acc = part_sum if acc is None else acc + part_sum
            parts = []
            for h in range(0, cw, HEAD):
                v = acc[:, h : h + HEAD]
                v = v - jnp.mean(v, axis=-1, keepdims=True)
                s = lax.rsqrt(jnp.mean(v * v, axis=-1, keepdims=True) + norm_floor)
                v = v * s * hgain[:, h : h + HEAD]
                parts.append(v * jax.nn.sigmoid(v))
            heads[pl.ds(base, sub), head_cols(t)] = jnp.concatenate(parts, axis=1).astype(BF16)
            return inner

        lax.fori_loop(0, chunk // sub, conv_step, 0)
        head_send(0, j, t, to_sib).start()
        head_send(1, j, t, to_y).start()
        return carry

    with jax.named_scope("mix"):
        lax.fori_loop(0, 4, mix_chunk, 0)
    with jax.named_scope("pass2"):
        pass_on(2, 0, 1, 2)
        pass_on(3, 0)

    def heads_on(j, carry):
        head_wait(1, j, ynb)
        head_send(2, j, ynb, to_sib).start()
        return carry

    with jax.named_scope("heads_on"):
        lax.fori_loop(0, 4, heads_on, 0)
    with jax.named_scope("coll2"):
        collect(2)

    def hid_block(seq, j, who):
        return hid.at[seq, rows(j), pl.ds(pl.multiple_of(who * ow, 128), ow)]

    def hid_send(kind, j, seq, who, where):
        block = hid_block(seq, j, who)
        return remote(block, block, es.at[kind, j], er.at[kind, j], where)

    def hid_wait(kind, j, seq, who):
        block = hid_block(seq, j, who)
        remote(block, block, es.at[kind, j], er.at[kind, j], to_sib).wait_recv()

    def out_chunk(j, carry):
        head_wait(0, j, sib)
        head_wait(2, j, far)
        own = tok[rows(j), pl.ds(pl.multiple_of(t * ow, 128), ow)].astype(F32)
        total = own + jnp.dot(heads[rows(j), :], wout[...], preferred_element_type=F32)
        hid[zl, rows(j), pl.ds(pl.multiple_of(t * ow, 128), ow)] = total.astype(BF16)
        hid_send(0, j, zl, t, to_sib).start()
        hid_send(1, j, zl, t, to_y).start()

        @pl.when(jnp.logical_not(middle))
        def _():
            hid_send(2, j, zl, t, to_z).start()

        return carry

    with jax.named_scope("outmm"):
        lax.fori_loop(0, 4, out_chunk, 0)
    with jax.named_scope("pass34a"):
        pass_on(4, 0)
        pass_on(3, 1)

    def hid_own(j, carry):
        hid_wait(1, j, zl, ynb)
        hid_send(3, j, zl, ynb, to_sib).start()
        return carry

    with jax.named_scope("hid_own"):
        lax.fori_loop(0, 4, hid_own, 0)
    with jax.named_scope("pass4b"):
        pass_on(4, 1)

    @pl.when(middle)
    def _():
        for j in range(4):
            hid_send(2, j, zl, t, to_z).start()

    with jax.named_scope("pass34c"):
        pass_on(3, 2)
        pass_on(4, 2)
    send_weights(5)
    with jax.named_scope("coll34"):
        collect(3, 4)

    freach = ff_taps.shape[0]
    ftap = ff_taps[:, pl.ds(pl.multiple_of(zl * hw, 128), hw)].astype(F32)
    asub = 32

    def ffn_chunk(i, carry):
        first = i < 4
        j = i % 4
        seq = jnp.where(first, zl, 1 - zl)

        @pl.when(first)
        def _():
            hid_wait(0, j, zl, sib)
            hid_wait(3, j, zl, far)

        @pl.when(jnp.logical_not(first))
        def _():
            hid_wait(4, j, 1 - zl, sib)
            hid_wait(6, j, 1 - zl, far)

        norm_rows(hid.at[seq, rows(j), :], xc, ffn_gain, chunk)
        gbuf[pl.ds(0, 8), :] = gbuf[pl.ds(chunk, 8), :]

        @pl.when(j == 0)
        def _():
            gbuf[pl.ds(0, 8), :] = jnp.zeros((8, hw), F32)

        gbuf[pl.ds(8, chunk), :] = jnp.dot(xc[...], wg[...], preferred_element_type=F32)
        ubuf[...] = jnp.dot(xc[...], wu[...], preferred_element_type=F32)

        def act(a, inner):
            base = pl.multiple_of(a * asub, asub)
            window = gbuf[pl.ds(base, asub + 8), :]
            acc = None
            for k in range(freach):
                o = 8 - (freach - 1) + k
                term = window[o : o + asub, :] * ftap[k : k + 1, :]
                acc = term if acc is None else acc + term
            v = acc * jax.nn.sigmoid(acc) * ubuf[pl.ds(base, asub), :]
            prod[pl.ds(pl.multiple_of(seq * length + j * chunk + base, asub), asub), :] = v.astype(BF16)
            return inner

        lax.fori_loop(0, chunk // asub, act, 0)

        @pl.when(first)
        def _():
            hid_wait(2, j, 1 - zl, t)
            hid_send(4, j, 1 - zl, t, to_sib).start()
            hid_send(5, j, 1 - zl, t, to_y).start()

        @pl.when((middle & (i == 3)) | (jnp.logical_not(middle) & (i == 7)))
        def _():
            pass_on(5, 0)

        @pl.when((i >= 1) & (i <= 4))
        def _():
            hid_wait(5, i - 1, 1 - zl, ynb)
            hid_send(6, i - 1, 1 - zl, ynb, to_sib).start()

        return carry

    with jax.named_scope("ffn"):
        lax.fori_loop(0, 8, ffn_chunk, 0)

    with jax.named_scope("own5"):
        own_copy(5).wait()
    blocks = 8

    def place(i):
        late = i // 4
        k = i % 4
        owner = jnp.where(late == 0, 2 * zh + k // 2, jnp.where(k % 2 == 0, 2 - zh, 3 - 3 * zh))
        flip = jnp.where(late == 0, k % 2, k // 2)
        half = jnp.where(flip == 0, r, 1 - r)
        return owner, flip, half

    def q1(i):
        return remote(part.at[i % 3, 1 - c], rs1.at[i], qs.at[0, i], qr.at[0, i], to_sib)

    def q2(i, fn):
        slot = i

        @pl.when(i % 2 == 0)
        def _():
            fn(remote(sum1.at[slot, 1 - y], rs2.at[i], qs.at[1, i], qr.at[1, i], to_y))

        @pl.when(i % 2 == 1)
        def _():
            fn(remote(sum1.at[slot, :, 1 - zl], rs2.at[i], qs.at[1, i], qr.at[1, i], to_z))

    def q3(i, fn):
        slot = i

        @pl.when(i % 2 == 0)
        def _():
            fn(remote(sum2.at[slot, 1 - zl], rs3.at[i], qs.at[2, i], qr.at[2, i], to_z))

        @pl.when(i % 2 == 1)
        def _():
            fn(remote(sum2.at[slot, 1 - y], rs3.at[i], qs.at[2, i], qr.at[2, i], to_y))

    def got(copy):
        copy.wait_recv()

    def sent(copy):
        copy.wait_send()

    def turn(i, carry):
        @pl.when((i == 2) | (i == 3))
        def _():
            owner = jnp.where(i == 2, 2 - zh, 3 - 3 * zh)
            z_arrived(5, owner)
            x_copy(5, owner).start()

        @pl.when(i < blocks)
        def _():
            owner, flip, half = place(i)

            @pl.when((owner != f) & (flip == 1))
            def _():
                x_arrived(5, owner)

            @pl.when(i >= 3)
            def _():
                q1(i - 3).wait_send()

            at = pl.ds(pl.multiple_of(owner * 2 * feat + half * feat, feat), feat)

            def block_rows(b, inner):
                cc, yy, ss = b // 4, (b // 2) % 2, b % 2
                row = pl.multiple_of(ss * length + (2 * yy + cc) * chunk, chunk)
                part[i % 3, cc, yy, ss] = lax.dot_general(
                    prod[pl.ds(row, chunk), :],
                    wd[at, :],
                    (((1,), (1,)), ((), ())),
                    preferred_element_type=F32,
                ).astype(BF16)
                return inner

            lax.fori_loop(0, 8, block_rows, 0)
            q1(i).start()

        @pl.when((i >= 1) & (i <= blocks))
        def _():
            n = i - 1
            q1(n).wait_recv()

            sum1[n] = (part[n % 3, c].astype(F32) + rs1[n].astype(F32)).astype(BF16)
            q2(n, start)

        @pl.when((i >= 3) & (i <= blocks + 2))
        def _():
            n = i - 3
            q2(n, got)


            @pl.when(n % 2 == 0)
            def _():
                sum2[n] = (sum1[n, y].astype(F32) + rs2[n].astype(F32)).astype(BF16)

            @pl.when(n % 2 == 1)
            def _():
                sum2[n] = (sum1[n, :, zl].astype(F32) + rs2[n].astype(F32)).astype(BF16)

            q3(n, start)

        @pl.when(i >= 5)
        def _():
            n = i - 5
            q3(n, got)
            mine = jnp.where(n % 2 == 0, zl, y)
            owner, flip, half = place(n)
            cols = pl.ds(pl.multiple_of(owner * 2 * feat + half * feat, feat), feat)
            base = hid[zl, pl.ds(pl.multiple_of(t * chunk, chunk), chunk), cols].astype(F32)
            total = base + (sum2[n, mine].astype(F32) + rs3[n].astype(F32))
            out[0, :, cols] = total.astype(BF16)

        return carry

    with jax.named_scope("rs"):
        lax.fori_loop(0, blocks + 5, turn, 0)

    for n in range(blocks):
        if n >= blocks - 3:
            q1(n).wait_send()
        q2(n, sent)
        q3(n, sent)

    for m in (2, 3, 4, 5):
        z_bulk(m, sent, lambda target: target >= 0)
    for m in (3, 4, 5):

        @pl.when(middle)
        def _():
            across(m).wait_send()

    @pl.when(f < 3)
    def _():
        for m in (0, 1):
            line_copy(m, f, f + 1, 4, True).wait_send()

    @pl.when(f > 0)
    def _():
        for m in (0, 1):
            line_copy(m, f, f - 1, 5, True).wait_send()

    for d in (1, 2, 3):
        for sign in (-1, 1):
            owner = f + sign * d
            after = f - sign

            @pl.when((owner >= 0) & (owner <= 3) & (after >= 0) & (after <= 3))
            def _():
                for m in (0, 1):
                    line_copy(m, owner, after, owner, False).wait_send()

    def drain(owner):
        for m in range(6):
            x_copy(m, owner).wait_send()

    others(drain)

    def drain_chunks(j, carry):
        head_send(0, j, t, to_sib).wait_send()
        head_send(1, j, t, to_y).wait_send()
        head_send(2, j, ynb, to_sib).wait_send()
        hid_send(0, j, zl, t, to_sib).wait_send()
        hid_send(1, j, zl, t, to_y).wait_send()
        hid_send(2, j, zl, t, to_z).wait_send()
        hid_send(3, j, zl, ynb, to_sib).wait_send()
        hid_send(4, j, 1 - zl, t, to_sib).wait_send()
        hid_send(5, j, 1 - zl, t, to_y).wait_send()
        hid_send(6, j, 1 - zl, ynb, to_sib).wait_send()
        return carry

    lax.fori_loop(0, 4, drain_chunks, 0)


def fused(*arrays):
    (tokens, mix_gain, value_w, gate_w, mix_taps, head_gain, out_w, ffn_gain, ffgate_w, up_w, ff_taps, down_w) = arrays
    _, length, width = tokens.shape
    fs = lax.axis_size("fs")
    cw, ow = value_w.shape[1], out_w.shape[1]
    hw = ffgate_w.shape[1] // 2
    chunk = length // 4
    feat = down_w.shape[0] // 2
    scratch = [
        pltpu.VMEM((length, width), BF16),
        pltpu.VMEM((length, width), BF16),
        pltpu.VMEM((fs * value_w.shape[0], 2 * cw), BF16),
        pltpu.VMEM((fs * out_w.shape[0], ow), BF16),
        pltpu.VMEM((length + 40, cw), F32),
        pltpu.VMEM((length, 4 * cw), BF16),
        pltpu.VMEM((2, length, width), BF16),
        pltpu.VMEM((chunk, width), BF16),
        pltpu.VMEM((8 * mix_taps.shape[0], cw), F32),
        pltpu.VMEM((fs * ffgate_w.shape[0], hw), BF16),
        pltpu.VMEM((fs * up_w.shape[0], hw), BF16),
        pltpu.VMEM((fs * down_w.shape[0], hw), BF16),
        pltpu.VMEM((chunk + 8, hw), F32),
        pltpu.VMEM((chunk, hw), F32),
        pltpu.VMEM((2 * length, hw), BF16),
        pltpu.VMEM((3, 2, 2, 2, chunk, feat), BF16),
        pltpu.VMEM((8, 2, 2, chunk, feat), BF16),
        pltpu.VMEM((8, 2, 2, chunk, feat), BF16),
        pltpu.VMEM((8, 2, chunk, feat), BF16),
        pltpu.VMEM((8, 2, chunk, feat), BF16),
        pltpu.VMEM((8, chunk, feat), BF16),
        pltpu.SemaphoreType.DMA((6,)),
        pltpu.SemaphoreType.DMA((4,)),
    ]
    scratch += [pltpu.SemaphoreType.DMA((6, n)) for n in (6, 4, 4, 4)]
    scratch += [pltpu.SemaphoreType.DMA((3, 4))] * 2
    scratch += [pltpu.SemaphoreType.DMA((7, 4))] * 2
    scratch += [pltpu.SemaphoreType.DMA((3, 8))] * 2
    anywhere = pl.BlockSpec(memory_space=pl.ANY)
    small = pl.BlockSpec(memory_space=pltpu.VMEM)
    return pl.pallas_call(
        kernel,
        out_shape=jax.ShapeDtypeStruct((1, chunk, width), BF16),
        in_specs=[anywhere, small, anywhere, anywhere, small, small, anywhere, small, anywhere, anywhere, small, anywhere],
        out_specs=small,
        scratch_shapes=scratch,
        compiler_params=pltpu.CompilerParams(
            collective_id=0, has_side_effects=True, vmem_limit_bytes=67043328
        ),
        name="layer",
    )(
        tokens,
        mix_gain,
        value_w,
        gate_w,
        mix_taps,
        head_gain,
        out_w,
        ffn_gain,
        ffgate_w,
        up_w,
        ff_taps,
        down_w,
    )


def solution(mesh):
    placed = (
        P(("rep", "fs"), None, None),
        P(),
        P("fs", "tp"),
        P("fs", "tp"),
        P(None, "tp"),
        P("tp"),
        P("fs", "tp"),
        P(),
        P("fs", "tp"),
        P("fs", "tp"),
        P(None, "tp"),
        P("fs", "tp"),
    )
    shape = mesh.shape
    small = shape["rep"] == 2 and shape["fs"] == 4 and shape["tp"] == 4
    return jax.shard_map(
        fused if small else plain,
        mesh=mesh,
        in_specs=placed,
        out_specs=P(("rep", "fs"), "tp", None),
        check_vma=False,
    )
```

```python
import functools

import jax
import jax.numpy as jnp
from jax import lax
from jax.experimental import pallas as pl
from jax.experimental.pallas import tpu as pltpu
from jax.sharding import PartitionSpec as P

HEAD = 128
MESH = pl.DeviceIdType.MESH
F32 = jnp.float32
BF16 = jnp.bfloat16
norm_floor = 0.01


def row_norm(floats_in, scales):
    floats = floats_in.astype(F32)
    scaled = floats * lax.rsqrt(jnp.mean(floats * floats, axis=-1, keepdims=True) + norm_floor)
    return (scaled * scales.astype(F32)).astype(BF16)


def causal_conv(signal, kernel_taps):
    reach = kernel_taps.shape[0]
    length = signal.shape[0]
    padded = jnp.pad(signal, ((reach - 1, 0), (0, 0)))
    summed = padded[0:length] * kernel_taps[0]
    for offset in range(1, reach):
        summed = summed + padded[offset : offset + length] * kernel_taps[offset]
    return summed


def head_norm(signal, scales):
    heads = []
    for start in range(0, signal.shape[1], HEAD):
        part = signal[:, start : start + HEAD]
        centre = part - jnp.mean(part, axis=-1, keepdims=True)
        spread = jnp.mean(centre * centre, axis=-1, keepdims=True)
        gain = scales[start : start + HEAD].astype(F32)
        heads.append(jax.nn.silu(centre * lax.rsqrt(spread + norm_floor) * gain))
    return jnp.concatenate(heads, axis=1).astype(BF16)


def plain(
    tokens,
    mix_gain,
    value_weight,
    gate_weight,
    mix_taps,
    head_gain,
    out_weight,
    ffn_gain,
    ffgate_weight,
    up_weight,
    ff_taps,
    down_weight,
):
    def rows_of(shard):
        return lax.all_gather(shard, "fs", axis=0, tiled=True)

    sequence = tokens[0]
    width = value_weight.shape[1]
    pair_full = rows_of(jnp.concatenate([value_weight, gate_weight], axis=1))
    out_full = rows_of(out_weight)
    normed = row_norm(sequence, mix_gain)
    both = jnp.dot(normed, pair_full, preferred_element_type=F32)
    glu_out = both[:, :width] * jax.nn.sigmoid(both[:, width:])
    mixed_pos = causal_conv(glu_out, mix_taps.astype(F32))
    head_out = head_norm(mixed_pos, head_gain)
    out_cols = out_full.shape[1]
    all_heads = lax.all_gather(head_out, "tp", axis=1, tiled=True)
    own_cols = lax.dynamic_slice_in_dim(sequence, lax.axis_index("tp") * out_cols, out_cols, 1)
    mixer_sum = jnp.dot(all_heads, out_full, preferred_element_type=F32)
    hidden_cols = (own_cols.astype(F32) + mixer_sum).astype(BF16)
    full_rows = lax.all_gather(hidden_cols, "tp", axis=1, tiled=True)
    normed_ffn = row_norm(full_rows, ffn_gain)
    ffgate = jnp.dot(normed_ffn, rows_of(ffgate_weight), preferred_element_type=F32)
    gated = jax.nn.silu(causal_conv(ffgate, ff_taps.astype(F32)))
    ff_up = jnp.dot(normed_ffn, rows_of(up_weight), preferred_element_type=F32)
    product = (gated * ff_up).astype(BF16)
    own_count = sequence.shape[0] // lax.axis_size("tp")
    own_rows = lax.dynamic_slice_in_dim(full_rows, lax.axis_index("tp") * own_count, own_count, 0)
    partial = lax.dot_general(
        product, rows_of(down_weight), (((1,), (1,)), ((), ())), preferred_element_type=F32
    )
    result = lax.psum_scatter(partial.astype(BF16), "tp", scatter_dimension=0, tiled=True)
    return (own_rows.astype(F32) + result.astype(F32)).astype(BF16)[None]


def kernel(
    tokens,
    mix_gain,
    value_w,
    gate_w,
    mix_taps,
    head_gain,
    out_w,
    ffn_gain,
    ffgate_w,
    up_w,
    ff_taps,
    down_w,
    out,
    tok,
    normed,
    wpair,
    wout,
    glu,
    heads,
    hid,
    tapb,
    wg,
    wu,
    wd,
    gbuf,
    ubuf,
    prod,
    part,
    rs1,
    sum1,
    rs2,
    sum2,
    rs3,
    loc,
    tsem,
    zs,
    zr,
    xs,
    xr,
    hs,
    hr,
    es,
    er,
    qs,
    qr,
):
    r, f, t = lax.axis_index("rep"), lax.axis_index("fs"), lax.axis_index("tp")
    y, c = t // 2, t % 2
    zl, zh = f % 2, f // 2
    fp = f + 1 - 2 * zl
    sib, ynb = t + 1 - 2 * c, (t + 2) % 4
    far = (sib + 2) % 4
    to_x, to_z, to_sib, to_y = {"rep": 1 - r}, {"fs": fp}, {"tp": sib}, {"tp": ynb}

    length, width = tok.shape
    chunk = length // 4
    cw = value_w.shape[1]
    ow = out_w.shape[1]
    hw = wg.shape[2]
    feat = down_w.shape[0] // 2

    def remote(src, dst, ss, rs, where):
        return pltpu.make_async_remote_copy(
            src_ref=src, dst_ref=dst, send_sem=ss, recv_sem=rs, device_id=where, device_id_type=MESH
        )

    barrier = pltpu.get_barrier_semaphore()
    for peer in (to_x, to_sib, to_y, {"fs": (f + 1) % 4}, {"fs": (f + 2) % 4}, {"fs": (f + 3) % 4}):
        pl.semaphore_signal(barrier, inc=1, device_id=peer, device_id_type=MESH)

    def rows(j):
        return pl.ds(pl.multiple_of(j * chunk, chunk), chunk)

    def tok_copy(j):
        return pltpu.make_async_copy(tokens.at[0, rows(j), :], tok.at[rows(j), :], tsem.at[j])

    for j in range(4):
        tok_copy(j).start()

    middle = (f == 1) | (f == 2)
    shares = jnp.where(middle, 2, 1)
    mats = (
        (value_w, wpair, 0, False),
        (gate_w, wpair, cw, False),
        (out_w, wout, 0, False),
        (ffgate_w, wg, 0, True),
        (up_w, wu, 0, True),
        (down_w, wd, None, True),
    )

    def is_middle(plane):
        return (plane == 1) | (plane == 2)

    def src_of(m, row, count, plane, share):
        w, dst, col, cut = mats[m]
        if cut:
            part_of = jnp.where(is_middle(plane), 1 + share, 0)
            return w.at[pl.ds(row, count), pl.ds(pl.multiple_of(part_of * hw, 128), hw)]
        return w.at[pl.ds(row, count), :]

    def dst_of(m, row, count, share):
        w, dst, col, cut = mats[m]
        if cut and col is None:
            return dst.at[pl.ds(row, count), pl.ds(share * hw, hw)]
        if cut:
            return dst.at[share, pl.ds(row, count), :]
        return dst.at[pl.ds(row, count), pl.ds(col, w.shape[1])]

    def piece(m, owner, half, share=0):
        n = mats[m][0].shape[0]
        return dst_of(m, pl.multiple_of(owner * n + half * (n // 2), n // 2), n // 2, share)

    def each_share(m, fn, plane=None):
        fn(0)
        if mats[m][3]:
            two = middle if plane is None else is_middle(plane)

            @pl.when(two)
            def _():
                fn(1)

    def own_copy(m, share):
        n = mats[m][0].shape[0]
        return pltpu.make_async_copy(
            src_of(m, 0, n, f, share), dst_of(m, pl.multiple_of(f * n, n), n, share), loc.at[m, share]
        )

    def z_copy(m, target, share):
        n = mats[m][0].shape[0]
        return remote(
            src_of(m, pl.multiple_of(r * (n // 2), n // 2), n // 2, target, share),
            piece(m, f, r, share),
            zs.at[m, target, share],
            zr.at[m, f, share],
            {"fs": target},
        )

    def z_arrived(m, owner, share=0):
        block = piece(m, owner, r, share)
        remote(block, block, zs.at[m, owner, share], zr.at[m, owner, share], to_x).wait_recv()

    def x_copy(m, owner, share=0):
        block = piece(m, owner, r, share)
        return remote(block, block, xs.at[m, owner, share], xr.at[m, owner, share], to_x)

    def x_arrived(m, owner, share=0):
        block = piece(m, owner, 1 - r, share)
        remote(block, block, xs.at[m, owner, share], xr.at[m, owner, share], to_x).wait_recv()

    def others(fn):
        def step(k, carry):
            fn(jnp.where(k == 0, fp, jnp.where(k == 1, 2 - zh, 3 - 3 * zh)))
            return carry

        lax.fori_loop(0, 3, step, 0)

    order = (fp, 2 - zh, 3 - 3 * zh)

    def line_copy(m, owner, target, slot, own):
        n = mats[m][0].shape[0]
        if own:
            src = src_of(m, pl.multiple_of(r * (n // 2), n // 2), n // 2, target, 0)
        else:
            src = piece(m, owner, r)
        return remote(src, piece(m, owner, r), zs.at[m, slot, 0], zr.at[m, owner, 0], {"fs": target})

    def z_bulk(m, fn, keep, shares_of=(0, 1)):
        def one(target):
            ok = keep(target)
            if mats[m][3]:
                ok = ok & (middle | (target != order[1]))

            for share in shares_of:
                if share == 1 and not mats[m][3]:
                    continue
                has = ok & is_middle(target) if share == 1 else ok

                @pl.when(has)
                def _():
                    fn(z_copy(m, target, share))

        others(one)

    def across(m, share):
        block = piece(m, fp, r, share)
        return remote(block, block, zs.at[m, f, share], zr.at[m, fp, share], {"fs": 3 - f})

    for m in range(6):
        each_share(m, lambda share: own_copy(m, share).start())
    with jax.named_scope("barrier"):
        pl.semaphore_wait(barrier, 6)

    def start(copy):
        copy.start()

    def every(target):
        return target >= 0

    def ends_only(target):
        return jnp.logical_not(is_middle(target))

    def pass_on(m, k, share):
        owner = order[k]
        z_arrived(m, owner, share)
        if mats[m][3] and k == 0:

            @pl.when(middle)
            def _():
                across(m, share).start()

        x_copy(m, owner, share).start()

    def relay(d):
        for sign in (-1, 1):
            owner = f + sign * d

            @pl.when((owner >= 0) & (owner <= 3))
            def _():
                for m in (0, 1):
                    z_arrived(m, owner)
                    after = f - sign

                    @pl.when((after >= 0) & (after <= 3))
                    def _():
                        line_copy(m, owner, after, owner, False).start()

                    x_copy(m, owner).start()


    def collect(share, *ms):
        def one(owner):
            for m in ms:
                x_arrived(m, owner, share)

        others(one)
        for m in ms:
            own_copy(m, share).wait()

    @pl.when(f < 3)
    def _():
        for m in (0, 1):
            line_copy(m, f, f + 1, 4, True).start()

    @pl.when(f > 0)
    def _():
        for m in (0, 1):
            line_copy(m, f, f - 1, 5, True).start()

    @pl.when(jnp.logical_not(middle))
    def _():
        for m in (3, 4):
            z_bulk(m, start, is_middle, (0,))

    def norm_rows(src, dst, gain_ref, count):
        gain = gain_ref[...].astype(F32).reshape(1, width)

        def step(i, carry):
            at = pl.ds(pl.multiple_of(i * 16, 16), 16)
            v = src[at, :].astype(F32)
            s = lax.rsqrt(jnp.mean(v * v, axis=-1, keepdims=True) + norm_floor)
            dst[at, :] = (v * s * gain).astype(BF16)
            return carry

        lax.fori_loop(0, count // 16, step, 0, unroll=4)

    glu[pl.ds(0, 32), :] = jnp.zeros((32, cw), F32)
    for k in range(mix_taps.shape[0]):
        tapb[pl.ds(8 * k, 8), :] = jnp.broadcast_to(mix_taps[k : k + 1, :].astype(F32), (8, mix_taps.shape[1]))
    with jax.named_scope("tokwait"):
        for j in range(4):
            tok_copy(j).wait()
        norm_rows(tok, normed, mix_gain, length)

    with jax.named_scope("pass01"):
        for d in (1, 2, 3):
            relay(d)
    with jax.named_scope("coll01"):
        collect(0, 0, 1)
    z_bulk(2, start, every)

    @pl.when(middle)
    def _():
        for m in (3, 4):
            z_bulk(m, start, is_middle, (0,))

    @pl.when(jnp.logical_not(middle))
    def _():
        for m in (3, 4):
            z_bulk(m, start, every, (1,))


    def head_cols(who):
        return pl.ds(pl.multiple_of(who * cw, 128), cw)

    def head_send(kind, j, who, where):
        block = heads.at[rows(j), head_cols(who)]
        return remote(block, block, hs.at[kind, j], hr.at[kind, j], where)

    def head_wait(kind, j, who):
        block = heads.at[rows(j), head_cols(who)]
        remote(block, block, hs.at[kind, j], hr.at[kind, j], to_sib).wait_recv()

    reach = mix_taps.shape[0]
    sub = 64

    hgain = head_gain[...].astype(F32).reshape(1, cw)

    def mix_chunk(j, carry):
        both = jnp.dot(normed[rows(j), :], wpair[...], preferred_element_type=F32)
        glu[pl.ds(pl.multiple_of(j * chunk + 32, 32), chunk), :] = both[:, :cw] * jax.nn.sigmoid(both[:, cw:])

        def conv_step(i, inner):
            base = pl.multiple_of(j * chunk + i * sub, sub)
            acc = None
            for e in range(8):
                rot = None
                for o in range(e, 33, 8):
                    k = o - (33 - reach)
                    if 0 <= k < reach:
                        view = glu[pl.ds(base + 8 * (o // 8), sub + 8), :].reshape(sub // 8 + 1, 8, cw)
                        term = view * tapb[pl.ds(8 * k, 8), :][None]
                        rot = term if rot is None else rot + term
                part_sum = rot.reshape(sub + 8, cw)[e : e + sub, :]
                acc = part_sum if acc is None else acc + part_sum
            parts = []
            for h in range(0, cw, HEAD):
                v = acc[:, h : h + HEAD]
                v = v - jnp.mean(v, axis=-1, keepdims=True)
                s = lax.rsqrt(jnp.mean(v * v, axis=-1, keepdims=True) + norm_floor)
                v = v * s * hgain[:, h : h + HEAD]
                parts.append(v * jax.nn.sigmoid(v))
            heads[pl.ds(base, sub), head_cols(t)] = jnp.concatenate(parts, axis=1).astype(BF16)
            return inner

        lax.fori_loop(0, chunk // sub, conv_step, 0)
        head_send(0, j, t, to_sib).start()
        head_send(1, j, t, to_y).start()
        return carry

    with jax.named_scope("mix"):
        lax.fori_loop(0, 4, mix_chunk, 0)
    with jax.named_scope("pass2"):
        for k in (0, 1, 2):
            pass_on(2, k, 0)

        @pl.when(middle)
        def _():
            for m in (3, 4):
                pass_on(m, 0, 0)

    def heads_on(j, carry):
        head_wait(1, j, ynb)
        head_send(2, j, ynb, to_sib).start()
        return carry

    with jax.named_scope("heads_on"):
        lax.fori_loop(0, 4, heads_on, 0)
    with jax.named_scope("coll2"):
        collect(0, 2)

    def hid_block(seq, j, who):
        return hid.at[seq, rows(j), pl.ds(pl.multiple_of(who * ow, 128), ow)]

    def hid_send(kind, j, seq, who, where):
        block = hid_block(seq, j, who)
        return remote(block, block, es.at[kind, j], er.at[kind, j], where)

    def hid_wait(kind, j, seq, who):
        block = hid_block(seq, j, who)
        remote(block, block, es.at[kind, j], er.at[kind, j], to_sib).wait_recv()

    def out_chunk(j, carry):
        head_wait(0, j, sib)
        head_wait(2, j, far)
        own = tok[rows(j), pl.ds(pl.multiple_of(t * ow, 128), ow)].astype(F32)
        total = own + jnp.dot(heads[rows(j), :], wout[...], preferred_element_type=F32)
        hid[zl, rows(j), pl.ds(pl.multiple_of(t * ow, 128), ow)] = total.astype(BF16)
        hid_send(0, j, zl, t, to_sib).start()
        hid_send(1, j, zl, t, to_y).start()

        @pl.when(jnp.logical_not(middle))
        def _():
            hid_send(2, j, zl, t, to_z).start()

        return carry

    with jax.named_scope("outmm"):
        lax.fori_loop(0, 4, out_chunk, 0)

    for m in (3, 4):
        z_bulk(m, start, ends_only, (0,))

    @pl.when(middle)
    def _():
        for j in range(4):
            hid_send(2, j, zl, t, to_z).start()
        for m in (3, 4):
            z_bulk(m, start, every, (1,))

    @pl.when(jnp.logical_not(middle))
    def _():
        z_bulk(5, start, is_middle)

    with jax.named_scope("pass1"):

        @pl.when(middle)
        def _():
            for m in (3, 4):
                pass_on(m, 1, 0)

    def hid_own(j, carry):
        hid_wait(1, j, zl, ynb)
        hid_send(3, j, zl, ynb, to_sib).start()

        @pl.when(middle & (j == 2))
        def _():
            for m in (3, 4):
                pass_on(m, 2, 0)

        @pl.when(jnp.logical_not(middle) & (j == 2))
        def _():
            for m in (3, 4):
                pass_on(m, 0, 0)

        return carry

    with jax.named_scope("hid_own"):
        lax.fori_loop(0, 4, hid_own, 0)

    with jax.named_scope("passE"):

        @pl.when(jnp.logical_not(middle))
        def _():
            for k in (1, 2):
                for m in (3, 4):
                    pass_on(m, k, 0)

    with jax.named_scope("pass0s1"):

        @pl.when(middle)
        def _():
            for m in (3, 4):
                pass_on(m, 0, 1)
            z_bulk(5, start, is_middle)

    def hid_partner(j, carry):
        hid_wait(2, j, 1 - zl, t)
        hid_send(4, j, 1 - zl, t, to_sib).start()
        hid_send(5, j, 1 - zl, t, to_y).start()
        return carry

    with jax.named_scope("hid_partner"):
        lax.fori_loop(0, 4, hid_partner, 0)
    with jax.named_scope("collect"):
        collect(0, 3, 4)

    freach = ff_taps.shape[0]
    asub = 32

    def ffn_rows(share, mine, j):
        seq = zl if mine else 1 - zl
        kept = normed if mine else tok
        if share == 0:
            norm_rows(hid.at[seq, rows(j), :], kept.at[rows(j), :], ffn_gain, chunk)
        xc = kept[rows(j), :]
        part_of = jnp.where(middle, 1 + share, 0)
        ftap = ff_taps[:, pl.ds(pl.multiple_of(part_of * hw, 128), hw)].astype(F32)
        gbuf[pl.ds(0, 8), :] = gbuf[pl.ds(chunk, 8), :]

        @pl.when(j == 0)
        def _():
            gbuf[pl.ds(0, 8), :] = jnp.zeros((8, hw), F32)

        gbuf[pl.ds(8, chunk), :] = jnp.dot(xc, wg[share], preferred_element_type=F32)
        ubuf[...] = jnp.dot(xc, wu[share], preferred_element_type=F32)

        def act(a, inner):
            base = pl.multiple_of(a * asub, asub)
            window = gbuf[pl.ds(base, asub + 8), :]
            acc = None
            for k in range(freach):
                o = 8 - (freach - 1) + k
                term = window[o : o + asub, :] * ftap[k : k + 1, :]
                acc = term if acc is None else acc + term
            v = acc * jax.nn.sigmoid(acc) * ubuf[pl.ds(base, asub), :]
            row = (4 * (j % 2) + 2 * (j // 2) + seq) * chunk + base
            prod[pl.ds(pl.multiple_of(row, asub), asub), share * hw : (share + 1) * hw] = v.astype(BF16)
            return inner

        lax.fori_loop(0, chunk // asub, act, 0)

    def ffn_own(j, carry):
        hid_wait(0, j, zl, sib)
        hid_wait(3, j, zl, far)
        ffn_rows(0, True, j)

        @pl.when(middle & (j == 3))
        def _():
            for m in (3, 4):
                pass_on(m, 1, 1)

        @pl.when(j >= 1)
        def _():
            hid_wait(5, j - 1, 1 - zl, ynb)
            hid_send(6, j - 1, 1 - zl, ynb, to_sib).start()

        return carry

    def ffn_partner(j, carry):
        @pl.when(j == 0)
        def _():
            hid_wait(5, 3, 1 - zl, ynb)
            hid_send(6, 3, 1 - zl, ynb, to_sib).start()

        hid_wait(4, j, 1 - zl, sib)
        hid_wait(6, j, 1 - zl, far)
        ffn_rows(0, False, j)

        @pl.when(middle & (j == 3))
        def _():
            for m in (3, 4):
                pass_on(m, 2, 1)

        return carry

    with jax.named_scope("ffn1"):
        lax.fori_loop(0, 4, ffn_own, 0)
        z_bulk(5, start, ends_only, (0,))
        lax.fori_loop(0, 4, ffn_partner, 0)

    def pass_down(k):
        each_share(5, lambda share: pass_on(5, k, share))

    def ffn_second(mine, k, j, carry):
        ffn_rows(1, mine, j)

        @pl.when(j == 0)
        def _():
            pass_down(k)

        return carry

    with jax.named_scope("ffn2"):

        @pl.when(middle)
        def _():
            collect(1, 3, 4)
            lax.fori_loop(0, 4, functools.partial(ffn_second, True, 0), 0)
            lax.fori_loop(0, 4, functools.partial(ffn_second, False, 1), 0)

    with jax.named_scope("own5"):
        each_share(5, lambda share: own_copy(5, share).wait())
    blocks = 8

    def place(i):
        late = i // 4
        k = i % 4
        owner = jnp.where(late == 0, jnp.where(k < 2, 3 * zh, 1 + zh), jnp.where(k % 2 == 0, 2 - zh, 3 - 3 * zh))
        flip = jnp.where(late == 0, k % 2, k // 2)
        half = jnp.where(flip == 0, r, 1 - r)
        return owner, flip, half

    def q1(i):
        return remote(part.at[i % 3, 1 - c], rs1.at[i], qs.at[0, i], qr.at[0, i], to_sib)

    def q2(i, fn):
        slot = i

        @pl.when(i % 2 == 0)
        def _():
            fn(remote(sum1.at[slot, 1 - y], rs2.at[i], qs.at[1, i], qr.at[1, i], to_y))

        @pl.when(i % 2 == 1)
        def _():
            fn(remote(sum1.at[slot, :, 1 - zl], rs2.at[i], qs.at[1, i], qr.at[1, i], to_z))

    def q3(i, fn):
        slot = i

        @pl.when(i % 2 == 0)
        def _():
            fn(remote(sum2.at[slot, 1 - zl], rs3.at[i], qs.at[2, i], qr.at[2, i], to_z))

        @pl.when(i % 2 == 1)
        def _():
            fn(remote(sum2.at[slot, 1 - y], rs3.at[i], qs.at[2, i], qr.at[2, i], to_y))

    def got(copy):
        copy.wait_recv()

    def sent(copy):
        copy.wait_send()

    def turn(i, carry):
        @pl.when((i == 1) & jnp.logical_not(middle))
        def _():
            pass_down(0)
            pass_down(1)

        @pl.when(i == 3)
        def _():
            pass_down(2)

        @pl.when(i < blocks)
        def _():
            owner, flip, half = place(i)

            @pl.when((owner != f) & (flip == 1))
            def _():
                each_share(5, lambda share: x_arrived(5, owner, share))

            @pl.when(i >= 3)
            def _():
                q1(i - 3).wait_send()

            at = pl.ds(pl.multiple_of(owner * 2 * feat + half * feat, feat), feat)

            def down(cc, units):
                return lax.dot_general(
                    prod[pl.ds(pl.multiple_of(cc * 4 * chunk, chunk), 4 * chunk), :units],
                    wd[at, :units],
                    (((1,), (1,)), ((), ())),
                    preferred_element_type=F32,
                ).astype(BF16)

            def down_rows(cc):
                @pl.when(middle)
                def _():
                    part[i % 3, cc] = down(cc, 2 * hw)

                @pl.when(jnp.logical_not(middle))
                def _():
                    part[i % 3, cc] = down(cc, hw)

            down_rows(1 - c)
            q1(i).start()
            down_rows(c)

        @pl.when((i >= 1) & (i <= blocks))
        def _():
            n = i - 1
            q1(n).wait_recv()

            total = (part[n % 3, c].astype(F32) + rs1[n].astype(F32)).astype(BF16)
            sum1[n] = total.reshape(2, 2, chunk, feat)
            q2(n, start)

        @pl.when((i >= 3) & (i <= blocks + 2))
        def _():
            n = i - 3
            q2(n, got)


            @pl.when(n % 2 == 0)
            def _():
                sum2[n] = (sum1[n, y].astype(F32) + rs2[n].astype(F32)).astype(BF16)

            @pl.when(n % 2 == 1)
            def _():
                sum2[n] = (sum1[n, :, zl].astype(F32) + rs2[n].astype(F32)).astype(BF16)

            q3(n, start)

        @pl.when(i >= 5)
        def _():
            n = i - 5
            q3(n, got)
            mine = jnp.where(n % 2 == 0, zl, y)
            owner, flip, half = place(n)
            cols = pl.ds(pl.multiple_of(owner * 2 * feat + half * feat, feat), feat)
            base = hid[zl, pl.ds(pl.multiple_of(t * chunk, chunk), chunk), cols].astype(F32)
            total = base + (sum2[n, mine].astype(F32) + rs3[n].astype(F32))
            out[0, :, cols] = total.astype(BF16)

        return carry

    with jax.named_scope("rs"):
        lax.fori_loop(0, blocks + 5, turn, 0)

    for n in range(blocks):
        if n >= blocks - 3:
            q1(n).wait_send()
        q2(n, sent)
        q3(n, sent)

    for m in (2, 3, 4, 5):
        z_bulk(m, sent, every)
    for m in (3, 4, 5):

        @pl.when(middle)
        def _():
            each_share(m, lambda share: across(m, share).wait_send())

    @pl.when(f < 3)
    def _():
        for m in (0, 1):
            line_copy(m, f, f + 1, 4, True).wait_send()

    @pl.when(f > 0)
    def _():
        for m in (0, 1):
            line_copy(m, f, f - 1, 5, True).wait_send()

    for d in (1, 2, 3):
        for sign in (-1, 1):
            owner = f + sign * d
            after = f - sign

            @pl.when((owner >= 0) & (owner <= 3) & (after >= 0) & (after <= 3))
            def _():
                for m in (0, 1):
                    line_copy(m, owner, after, owner, False).wait_send()

    def drain(owner):
        for m in range(6):
            each_share(m, lambda share: x_copy(m, owner, share).wait_send())

    others(drain)

    def drain_chunks(j, carry):
        head_send(0, j, t, to_sib).wait_send()
        head_send(1, j, t, to_y).wait_send()
        head_send(2, j, ynb, to_sib).wait_send()
        hid_send(0, j, zl, t, to_sib).wait_send()
        hid_send(1, j, zl, t, to_y).wait_send()
        hid_send(2, j, zl, t, to_z).wait_send()
        hid_send(3, j, zl, ynb, to_sib).wait_send()
        hid_send(4, j, 1 - zl, t, to_sib).wait_send()
        hid_send(5, j, 1 - zl, t, to_y).wait_send()
        hid_send(6, j, 1 - zl, ynb, to_sib).wait_send()
        return carry

    lax.fori_loop(0, 4, drain_chunks, 0)


def fused(*arrays):
    (tokens, mix_gain, value_w, gate_w, mix_taps, head_gain, out_w, ffn_gain, ffgate_w, up_w, ff_taps, down_w) = arrays
    _, length, width = tokens.shape
    fs = lax.axis_size("fs")
    cw, ow = value_w.shape[1], out_w.shape[1]
    hw = ffgate_w.shape[1] // 3
    chunk = length // 4
    feat = down_w.shape[0] // 2
    scratch = [
        pltpu.VMEM((length, width), BF16),
        pltpu.VMEM((length, width), BF16),
        pltpu.VMEM((fs * value_w.shape[0], 2 * cw), BF16),
        pltpu.VMEM((fs * out_w.shape[0], ow), BF16),
        pltpu.VMEM((length + 40, cw), F32),
        pltpu.VMEM((length, 4 * cw), BF16),
        pltpu.VMEM((2, length, width), BF16),
        pltpu.VMEM((8 * mix_taps.shape[0], cw), F32),
        pltpu.VMEM((2, fs * ffgate_w.shape[0], hw), BF16),
        pltpu.VMEM((2, fs * up_w.shape[0], hw), BF16),
        pltpu.VMEM((fs * down_w.shape[0], 2 * hw), BF16),
        pltpu.VMEM((chunk + 8, hw), F32),
        pltpu.VMEM((chunk, hw), F32),
        pltpu.VMEM((2 * length, 2 * hw), BF16),
        pltpu.VMEM((3, 2, 4 * chunk, feat), BF16),
        pltpu.VMEM((8, 4 * chunk, feat), BF16),
        pltpu.VMEM((8, 2, 2, chunk, feat), BF16),
        pltpu.VMEM((8, 2, chunk, feat), BF16),
        pltpu.VMEM((8, 2, chunk, feat), BF16),
        pltpu.VMEM((8, chunk, feat), BF16),
        pltpu.SemaphoreType.DMA((6, 2)),
        pltpu.SemaphoreType.DMA((4,)),
    ]
    scratch += [pltpu.SemaphoreType.DMA((6, n, 2)) for n in (6, 4, 4, 4)]
    scratch += [pltpu.SemaphoreType.DMA((3, 4))] * 2
    scratch += [pltpu.SemaphoreType.DMA((7, 4))] * 2
    scratch += [pltpu.SemaphoreType.DMA((3, 8))] * 2
    anywhere = pl.BlockSpec(memory_space=pl.ANY)
    small = pl.BlockSpec(memory_space=pltpu.VMEM)
    return pl.pallas_call(
        kernel,
        out_shape=jax.ShapeDtypeStruct((1, chunk, width), BF16),
        in_specs=[anywhere, small, anywhere, anywhere, small, small, anywhere, small, anywhere, anywhere, small, anywhere],
        out_specs=small,
        scratch_shapes=scratch,
        compiler_params=pltpu.CompilerParams(
            collective_id=0, has_side_effects=True, vmem_limit_bytes=67043328
        ),
        name="layer",
    )(
        tokens,
        mix_gain,
        value_w,
        gate_w,
        mix_taps,
        head_gain,
        out_w,
        ffn_gain,
        ffgate_w,
        up_w,
        ff_taps,
        down_w,
    )


def solution(mesh):
    placed = (
        P(("rep", "fs"), None, None),
        P(),
        P("fs", "tp"),
        P("fs", "tp"),
        P(None, "tp"),
        P("tp"),
        P("fs", "tp"),
        P(),
        P("fs", "tp"),
        P("fs", "tp"),
        P(None, "tp"),
        P("fs", "tp"),
    )
    shape = mesh.shape
    small = shape["rep"] == 2 and shape["fs"] == 4 and shape["tp"] == 4
    return jax.shard_map(
        fused if small else plain,
        mesh=mesh,
        in_specs=placed,
        out_specs=P(("rep", "fs"), "tp", None),
        check_vma=False,
    )
```

```python
import functools

import jax
import jax.numpy as jnp
from jax import lax
from jax.experimental import pallas as pl
from jax.experimental.pallas import tpu as pltpu
from jax.sharding import PartitionSpec as P

HEAD = 128
MESH = pl.DeviceIdType.MESH
F32 = jnp.float32
BF16 = jnp.bfloat16
norm_floor = 0.01


def row_norm(floats_in, scales):
    floats = floats_in.astype(F32)
    scaled = floats * lax.rsqrt(jnp.mean(floats * floats, axis=-1, keepdims=True) + norm_floor)
    return (scaled * scales.astype(F32)).astype(BF16)


def causal_conv(signal, kernel_taps):
    reach = kernel_taps.shape[0]
    length = signal.shape[0]
    padded = jnp.pad(signal, ((reach - 1, 0), (0, 0)))
    summed = padded[0:length] * kernel_taps[0]
    for offset in range(1, reach):
        summed = summed + padded[offset : offset + length] * kernel_taps[offset]
    return summed


def head_norm(signal, scales):
    heads = []
    for start in range(0, signal.shape[1], HEAD):
        part = signal[:, start : start + HEAD]
        centre = part - jnp.mean(part, axis=-1, keepdims=True)
        spread = jnp.mean(centre * centre, axis=-1, keepdims=True)
        gain = scales[start : start + HEAD].astype(F32)
        heads.append(jax.nn.silu(centre * lax.rsqrt(spread + norm_floor) * gain))
    return jnp.concatenate(heads, axis=1).astype(BF16)


def plain(
    tokens,
    mix_gain,
    value_weight,
    gate_weight,
    mix_taps,
    head_gain,
    out_weight,
    ffn_gain,
    ffgate_weight,
    up_weight,
    ff_taps,
    down_weight,
):
    def rows_of(shard):
        return lax.all_gather(shard, "fs", axis=0, tiled=True)

    sequence = tokens[0]
    width = value_weight.shape[1]
    pair_full = rows_of(jnp.concatenate([value_weight, gate_weight], axis=1))
    out_full = rows_of(out_weight)
    normed = row_norm(sequence, mix_gain)
    both = jnp.dot(normed, pair_full, preferred_element_type=F32)
    glu_out = both[:, :width] * jax.nn.sigmoid(both[:, width:])
    mixed_pos = causal_conv(glu_out, mix_taps.astype(F32))
    head_out = head_norm(mixed_pos, head_gain)
    out_cols = out_full.shape[1]
    all_heads = lax.all_gather(head_out, "tp", axis=1, tiled=True)
    own_cols = lax.dynamic_slice_in_dim(sequence, lax.axis_index("tp") * out_cols, out_cols, 1)
    mixer_sum = jnp.dot(all_heads, out_full, preferred_element_type=F32)
    hidden_cols = (own_cols.astype(F32) + mixer_sum).astype(BF16)
    full_rows = lax.all_gather(hidden_cols, "tp", axis=1, tiled=True)
    normed_ffn = row_norm(full_rows, ffn_gain)
    ffgate = jnp.dot(normed_ffn, rows_of(ffgate_weight), preferred_element_type=F32)
    gated = jax.nn.silu(causal_conv(ffgate, ff_taps.astype(F32)))
    ff_up = jnp.dot(normed_ffn, rows_of(up_weight), preferred_element_type=F32)
    product = (gated * ff_up).astype(BF16)
    own_count = sequence.shape[0] // lax.axis_size("tp")
    own_rows = lax.dynamic_slice_in_dim(full_rows, lax.axis_index("tp") * own_count, own_count, 0)
    partial = lax.dot_general(
        product, rows_of(down_weight), (((1,), (1,)), ((), ())), preferred_element_type=F32
    )
    result = lax.psum_scatter(partial.astype(BF16), "tp", scatter_dimension=0, tiled=True)
    return (own_rows.astype(F32) + result.astype(F32)).astype(BF16)[None]


def kernel(
    tokens,
    mix_gain,
    value_w,
    gate_w,
    mix_taps,
    head_gain,
    out_w,
    ffn_gain,
    ffgate_w,
    up_w,
    ff_taps,
    down_w,
    out,
    tok,
    normed,
    wpair,
    wout,
    glu,
    heads,
    hid,
    tapb,
    wg,
    wu,
    wd,
    gbuf,
    prod,
    part,
    rs1,
    sum1,
    rs2,
    sum2,
    rs3,
    outv,
    osem,
    loc,
    tsem,
    zs,
    zr,
    xs,
    xr,
    hs,
    hr,
    es,
    er,
    qs,
    qr,
):
    r, f, t = lax.axis_index("rep"), lax.axis_index("fs"), lax.axis_index("tp")
    y, c = t // 2, t % 2
    zl, zh = f % 2, f // 2
    fp = f + 1 - 2 * zl
    sib, ynb = t + 1 - 2 * c, (t + 2) % 4
    far = (sib + 2) % 4
    to_x, to_z, to_sib, to_y = {"rep": 1 - r}, {"fs": fp}, {"tp": sib}, {"tp": ynb}

    length, width = tok.shape
    chunk = length // 4
    cw = value_w.shape[1]
    ow = out_w.shape[1]
    hw = wg.shape[2]
    feat = down_w.shape[0] // 2

    def remote(src, dst, ss, rs, where):
        return pltpu.make_async_remote_copy(
            src_ref=src, dst_ref=dst, send_sem=ss, recv_sem=rs, device_id=where, device_id_type=MESH
        )

    barrier = pltpu.get_barrier_semaphore()
    for peer in (to_x, to_sib, to_y, {"fs": (f + 1) % 4}, {"fs": (f + 2) % 4}, {"fs": (f + 3) % 4}):
        pl.semaphore_signal(barrier, inc=1, device_id=peer, device_id_type=MESH)

    def rows(j):
        return pl.ds(pl.multiple_of(j * chunk, chunk), chunk)

    def tok_copy(j):
        return pltpu.make_async_copy(tokens.at[0, rows(j), :], tok.at[rows(j), :], tsem.at[j])

    for j in range(4):
        tok_copy(j).start()

    middle = (f == 1) | (f == 2)
    shares = jnp.where(middle, 2, 1)
    mats = (
        (value_w, wpair, 0, False),
        (gate_w, wpair, cw, False),
        (out_w, wout, 0, False),
        (ffgate_w, wg, 0, True),
        (up_w, wu, 0, True),
        (down_w, wd, None, True),
    )

    def is_middle(plane):
        return (plane == 1) | (plane == 2)

    def src_of(m, row, count, plane, share):
        w, dst, col, cut = mats[m]
        if cut:
            part_of = jnp.where(is_middle(plane), 1 + share, 0)
            return w.at[pl.ds(row, count), pl.ds(pl.multiple_of(part_of * hw, 128), hw)]
        return w.at[pl.ds(row, count), :]

    def dst_of(m, row, count, share):
        w, dst, col, cut = mats[m]
        if cut and col is None:
            return dst.at[pl.ds(row, count), pl.ds(share * hw, hw)]
        if cut:
            return dst.at[share, pl.ds(row, count), :]
        return dst.at[pl.ds(row, count), pl.ds(col, w.shape[1])]

    def piece(m, owner, half, share=0):
        n = mats[m][0].shape[0]
        return dst_of(m, pl.multiple_of(owner * n + half * (n // 2), n // 2), n // 2, share)

    def each_share(m, fn, plane=None):
        fn(0)
        if mats[m][3]:
            two = middle if plane is None else is_middle(plane)

            @pl.when(two)
            def _():
                fn(1)

    def own_copy(m, share):
        n = mats[m][0].shape[0]
        return pltpu.make_async_copy(
            src_of(m, 0, n, f, share), dst_of(m, pl.multiple_of(f * n, n), n, share), loc.at[m, share]
        )

    def z_copy(m, target, share):
        n = mats[m][0].shape[0]
        return remote(
            src_of(m, pl.multiple_of(r * (n // 2), n // 2), n // 2, target, share),
            piece(m, f, r, share),
            zs.at[m, target, share],
            zr.at[m, f, share],
            {"fs": target},
        )

    def z_arrived(m, owner, share=0):
        block = piece(m, owner, r, share)
        remote(block, block, zs.at[m, owner, share], zr.at[m, owner, share], to_x).wait_recv()

    def x_copy(m, owner, share=0):
        block = piece(m, owner, r, share)
        return remote(block, block, xs.at[m, owner, share], xr.at[m, owner, share], to_x)

    def x_arrived(m, owner, share=0):
        block = piece(m, owner, 1 - r, share)
        remote(block, block, xs.at[m, owner, share], xr.at[m, owner, share], to_x).wait_recv()

    def others(fn):
        def step(k, carry):
            fn(jnp.where(k == 0, fp, jnp.where(k == 1, 2 - zh, 3 - 3 * zh)))
            return carry

        lax.fori_loop(0, 3, step, 0)

    order = (fp, 2 - zh, 3 - 3 * zh)

    def line_copy(m, owner, target, slot, own):
        n = mats[m][0].shape[0]
        if own:
            src = src_of(m, pl.multiple_of(r * (n // 2), n // 2), n // 2, target, 0)
        else:
            src = piece(m, owner, r)
        return remote(src, piece(m, owner, r), zs.at[m, slot, 0], zr.at[m, owner, 0], {"fs": target})

    def z_bulk(m, fn, keep, shares_of=(0, 1)):
        def one(target):
            ok = keep(target)
            if mats[m][3]:
                ok = ok & (middle | (target != order[1]))

            for share in shares_of:
                if share == 1 and not mats[m][3]:
                    continue
                has = ok & is_middle(target) if share == 1 else ok

                @pl.when(has)
                def _():
                    fn(z_copy(m, target, share))

        others(one)

    def across(m, share):
        block = piece(m, fp, r, share)
        return remote(block, block, zs.at[m, f, share], zr.at[m, fp, share], {"fs": 3 - f})

    for m in range(6):
        each_share(m, lambda share: own_copy(m, share).start())
    with jax.named_scope("barrier"):
        pl.semaphore_wait(barrier, 6)

    def start(copy):
        copy.start()

    def every(target):
        return target >= 0

    def ends_only(target):
        return jnp.logical_not(is_middle(target))

    def pass_on(m, k, share):
        owner = order[k]
        z_arrived(m, owner, share)
        if mats[m][3] and k == 0:

            @pl.when(middle)
            def _():
                across(m, share).start()

        x_copy(m, owner, share).start()

    def relay(d):
        for sign in (-1, 1):
            owner = f + sign * d

            @pl.when((owner >= 0) & (owner <= 3))
            def _():
                for m in (0, 1):
                    z_arrived(m, owner)
                    after = f - sign

                    @pl.when((after >= 0) & (after <= 3))
                    def _():
                        line_copy(m, owner, after, owner, False).start()

                    x_copy(m, owner).start()


    def collect(share, *ms):
        def one(owner):
            for m in ms:
                x_arrived(m, owner, share)

        others(one)
        for m in ms:
            own_copy(m, share).wait()

    @pl.when(f < 3)
    def _():
        for m in (0, 1):
            line_copy(m, f, f + 1, 4, True).start()

    @pl.when(f > 0)
    def _():
        for m in (0, 1):
            line_copy(m, f, f - 1, 5, True).start()

    @pl.when(jnp.logical_not(middle))
    def _():
        for m in (3, 4):
            z_bulk(m, start, is_middle, (0,))

    def norm_rows(src, dst, gain_ref, count):
        gain = gain_ref[...].astype(F32).reshape(1, width)

        def step(i, carry):
            at = pl.ds(pl.multiple_of(i * 16, 16), 16)
            v = src[at, :].astype(F32)
            s = lax.rsqrt(jnp.mean(v * v, axis=-1, keepdims=True) + norm_floor)
            dst[at, :] = (v * s * gain).astype(BF16)
            return carry

        lax.fori_loop(0, count // 16, step, 0, unroll=4)

    glu[pl.ds(0, 32), :] = jnp.zeros((32, cw), F32)
    for k in range(mix_taps.shape[0]):
        tapb[pl.ds(8 * k, 8), :] = jnp.broadcast_to(mix_taps[k : k + 1, :].astype(F32), (8, mix_taps.shape[1]))
    with jax.named_scope("tokwait"):
        for j in range(4):
            tok_copy(j).wait()
        norm_rows(tok, normed, mix_gain, length)

    with jax.named_scope("pass01"):
        for d in (1, 2, 3):
            relay(d)
    @pl.when(middle)
    def _():
        for m in (3, 4):
            z_bulk(m, start, is_middle, (0,))

    with jax.named_scope("coll01"):
        collect(0, 0, 1)
    z_bulk(2, start, every)

    @pl.when(jnp.logical_not(middle))
    def _():
        for m in (3, 4):
            z_bulk(m, start, every, (1,))


    def head_cols(who):
        return pl.ds(pl.multiple_of(who * cw, 128), cw)

    def head_send(kind, j, who, where):
        block = heads.at[rows(j), head_cols(who)]
        return remote(block, block, hs.at[kind, j], hr.at[kind, j], where)

    def head_wait(kind, j, who):
        block = heads.at[rows(j), head_cols(who)]
        remote(block, block, hs.at[kind, j], hr.at[kind, j], to_sib).wait_recv()

    reach = mix_taps.shape[0]
    sub = 64

    hgain = head_gain[...].astype(F32).reshape(1, cw)

    def mix_chunk(j, carry):
        both = jnp.dot(normed[rows(j), :], wpair[...], preferred_element_type=F32)
        glu[pl.ds(pl.multiple_of(j * chunk + 32, 32), chunk), :] = both[:, :cw] * jax.nn.sigmoid(both[:, cw:])

        def conv_step(i, inner):
            base = pl.multiple_of(j * chunk + i * sub, sub)
            acc = None
            for e in range(8):
                rot = None
                for o in range(e, 33, 8):
                    k = o - (33 - reach)
                    if 0 <= k < reach:
                        view = glu[pl.ds(base + 8 * (o // 8), sub + 8), :].reshape(sub // 8 + 1, 8, cw)
                        term = view * tapb[pl.ds(8 * k, 8), :][None]
                        rot = term if rot is None else rot + term
                part_sum = rot.reshape(sub + 8, cw)[e : e + sub, :]
                acc = part_sum if acc is None else acc + part_sum
            parts = []
            for h in range(0, cw, HEAD):
                v = acc[:, h : h + HEAD]
                v = v - jnp.mean(v, axis=-1, keepdims=True)
                s = lax.rsqrt(jnp.mean(v * v, axis=-1, keepdims=True) + norm_floor)
                v = v * s * hgain[:, h : h + HEAD]
                parts.append(v * jax.nn.sigmoid(v))
            heads[pl.ds(base, sub), head_cols(t)] = jnp.concatenate(parts, axis=1).astype(BF16)
            return inner

        lax.fori_loop(0, chunk // sub, conv_step, 0)
        head_send(0, j, t, to_sib).start()
        head_send(1, j, t, to_y).start()
        return carry

    with jax.named_scope("mix"):
        lax.fori_loop(0, 4, mix_chunk, 0)
    with jax.named_scope("pass2"):
        for k in (0, 1, 2):
            pass_on(2, k, 0)

        @pl.when(middle)
        def _():
            for m in (3, 4):
                pass_on(m, 0, 0)

    @pl.when(middle)
    def _():
        for m in (3, 4):
            z_bulk(m, start, lambda target: target == fp, (0,))

    def heads_on(j, carry):
        head_wait(1, j, ynb)
        head_send(2, j, ynb, to_sib).start()
        return carry

    with jax.named_scope("heads_on"):
        lax.fori_loop(0, 4, heads_on, 0)
    with jax.named_scope("coll2"):
        collect(0, 2)

    def hid_block(seq, j, who):
        return hid.at[seq, rows(j), pl.ds(pl.multiple_of(who * ow, 128), ow)]

    def hid_send(kind, j, seq, who, where):
        block = hid_block(seq, j, who)
        return remote(block, block, es.at[kind, j], er.at[kind, j], where)

    def hid_wait(kind, j, seq, who):
        block = hid_block(seq, j, who)
        remote(block, block, es.at[kind, j], er.at[kind, j], to_sib).wait_recv()

    def out_chunk(j, carry):
        head_wait(0, j, sib)
        head_wait(2, j, far)
        own = tok[rows(j), pl.ds(pl.multiple_of(t * ow, 128), ow)].astype(F32)
        total = own + jnp.dot(heads[rows(j), :], wout[...], preferred_element_type=F32)
        hid[zl, rows(j), pl.ds(pl.multiple_of(t * ow, 128), ow)] = total.astype(BF16)
        hid_send(0, j, zl, t, to_sib).start()
        hid_send(1, j, zl, t, to_y).start()

        @pl.when(jnp.logical_not(middle))
        def _():
            hid_send(2, j, zl, t, to_z).start()

        return carry

    with jax.named_scope("outmm"):
        lax.fori_loop(0, 4, out_chunk, 0)

    for m in (3, 4):
        z_bulk(m, start, lambda target: ends_only(target) & (target != fp), (0,))

    @pl.when(middle)
    def _():
        for j in range(4):
            hid_send(2, j, zl, t, to_z).start()
        for m in (3, 4):
            z_bulk(m, start, every, (1,))

    @pl.when(jnp.logical_not(middle))
    def _():
        z_bulk(5, start, is_middle)

    with jax.named_scope("pass1"):

        @pl.when(middle)
        def _():
            for m in (3, 4):
                pass_on(m, 1, 0)

        @pl.when(jnp.logical_not(middle))
        def _():
            for m in (3, 4):
                pass_on(m, 0, 0)

    def hid_own(j, carry):
        hid_wait(1, j, zl, ynb)
        hid_send(3, j, zl, ynb, to_sib).start()

        @pl.when(middle & (j == 2))
        def _():
            for m in (3, 4):
                pass_on(m, 2, 0)

        return carry

    with jax.named_scope("hid_own"):
        lax.fori_loop(0, 4, hid_own, 0)

    with jax.named_scope("passE"):

        @pl.when(jnp.logical_not(middle))
        def _():
            for k in (1, 2):
                for m in (3, 4):
                    pass_on(m, k, 0)

    with jax.named_scope("pass0s1"):

        @pl.when(middle)
        def _():
            for m in (3, 4):
                pass_on(m, 0, 1)
            z_bulk(5, start, is_middle)

    def hid_partner(j, carry):
        hid_wait(2, j, 1 - zl, t)
        hid_send(4, j, 1 - zl, t, to_sib).start()
        hid_send(5, j, 1 - zl, t, to_y).start()
        return carry

    freach = ff_taps.shape[0]
    asub = 32

    def kept_rows(mine, j):
        return (normed if mine else tok)[rows(j), :]

    def prod_row(mine, j):
        seq = zl if mine else 1 - zl
        return pl.multiple_of((4 * (j % 2) + 2 * (j // 2) + seq) * chunk, chunk)

    def gate_rows(share, mine, j):
        if share == 0:
            kept = normed if mine else tok
            seq = zl if mine else 1 - zl
            norm_rows(hid.at[seq, rows(j), :], kept.at[rows(j), :], ffn_gain, chunk)
        part_of = jnp.where(middle, 1 + share, 0)
        ftap = ff_taps[:, pl.ds(pl.multiple_of(part_of * hw, 128), hw)].astype(F32)
        gbuf[pl.ds(0, 8), :] = gbuf[pl.ds(chunk, 8), :]

        @pl.when(j == 0)
        def _():
            gbuf[pl.ds(0, 8), :] = jnp.zeros((8, hw), F32)

        gbuf[pl.ds(8, chunk), :] = jnp.dot(kept_rows(mine, j), wg[share], preferred_element_type=F32)

        def act(a, inner):
            base = pl.multiple_of(a * asub, asub)
            window = gbuf[pl.ds(base, asub + 8), :]
            acc = None
            for k in range(freach):
                o = 8 - (freach - 1) + k
                term = window[o : o + asub, :] * ftap[k : k + 1, :]
                acc = term if acc is None else acc + term
            gated = (acc * jax.nn.sigmoid(acc)).astype(BF16)
            prod[pl.ds(prod_row(mine, j) + base, asub), share * hw : (share + 1) * hw] = gated
            return inner

        lax.fori_loop(0, chunk // asub, act, 0)

    def up_rows(share, mine, j):
        at = pl.ds(prod_row(mine, j), chunk)
        cols = slice(share * hw, (share + 1) * hw)
        ff_up = jnp.dot(kept_rows(mine, j), wu[share], preferred_element_type=F32)
        prod[at, cols] = (prod[at, cols].astype(F32) * ff_up).astype(BF16)

    def pass_down(k):
        each_share(5, lambda share: pass_on(5, k, share))

    def hid_last(j):
        hid_wait(5, j, 1 - zl, ynb)
        hid_send(6, j, 1 - zl, ynb, to_sib).start()

    def own_ready(j):
        hid_wait(0, j, zl, sib)
        hid_wait(3, j, zl, far)

    def partner_ready(j):
        hid_wait(4, j, 1 - zl, sib)
        hid_wait(6, j, 1 - zl, far)

    def four(fn):
        def step(j, carry):
            fn(j)
            return carry

        lax.fori_loop(0, 4, step, 0)

    @pl.when(middle)
    def _():
        with jax.named_scope("hid_partner"):
            lax.fori_loop(0, 4, hid_partner, 0)
        with jax.named_scope("collect"):
            collect(0, 3, 4)

        def own(j):
            own_ready(j)
            gate_rows(0, True, j)
            up_rows(0, True, j)
            pl.when(j >= 1)(lambda: hid_last(j - 1))

        def partner(j):
            pl.when(j == 0)(lambda: hid_last(3))
            partner_ready(j)
            gate_rows(0, False, j)
            up_rows(0, False, j)

        with jax.named_scope("ffn1"):
            four(own)
            for m in (3, 4):
                pass_on(m, 1, 1)
            z_bulk(5, start, ends_only, (0,))
            four(partner)
        with jax.named_scope("coll1g"):
            pass_on(3, 2, 1)
            collect(1, 3)

        def own_gate(j):
            gate_rows(1, True, j)
            pl.when(j == 1)(lambda: pass_on(4, 2, 1))

        with jax.named_scope("gate2"):
            four(own_gate)
            pass_down(0)
            four(lambda j: gate_rows(1, False, j))
        with jax.named_scope("coll1u"):
            collect(1, 4)
        with jax.named_scope("up2"):
            four(lambda j: up_rows(1, True, j))
            pass_down(1)
            four(lambda j: up_rows(1, False, j))

    @pl.when(jnp.logical_not(middle))
    def _():
        with jax.named_scope("hid_partner"):
            lax.fori_loop(0, 2, hid_partner, 0)
        with jax.named_scope("collect"):
            collect(0, 3)

        def own_gate(j):
            own_ready(j)
            gate_rows(0, True, j)
            pl.when(j < 2)(lambda: hid_partner(j + 2, None))
            pl.when(j == 2)(lambda: hid_last(0))

        with jax.named_scope("gate1"):
            four(own_gate)
        with jax.named_scope("coll0u"):
            collect(0, 4)
            z_bulk(5, start, ends_only, (0,))

        def partner(j):
            partner_ready(j)
            gate_rows(0, False, j)
            up_rows(0, False, j)
            pl.when(j == 0)(lambda: hid_last(3))
            pl.when(j == 2)(lambda: pass_down(0))

        with jax.named_scope("up1"):
            four(lambda j: up_rows(0, True, j))
            hid_last(1)
            hid_last(2)
        with jax.named_scope("ffnp"):
            four(partner)

    with jax.named_scope("own5"):
        each_share(5, lambda share: own_copy(5, share).wait())
    blocks = 8

    def place(i):
        late = i // 4
        k = i % 4
        flip = k // 2
        early_owner = jnp.where(k % 2 == 0, 3 * zh, 1 + zh)
        late_owner = jnp.where(k % 2 == 0, 2 - zh, 3 - 3 * zh)
        owner = jnp.where(late == 0, early_owner, late_owner)
        half = jnp.where(flip == 0, r, 1 - r)
        return owner, flip, half

    def q1(i):
        return remote(part.at[i % 3, 1 - c], rs1.at[i], qs.at[0, i], qr.at[0, i], to_sib)

    def q2(i, fn):
        slot = i

        @pl.when(i % 2 == 1)
        def _():
            fn(remote(sum1.at[slot, 1 - y], rs2.at[i], qs.at[1, i], qr.at[1, i], to_y))

        @pl.when(i % 2 == 0)
        def _():
            fn(remote(sum1.at[slot, :, 1 - zl], rs2.at[i], qs.at[1, i], qr.at[1, i], to_z))

    def q3(i, fn):
        slot = i

        @pl.when(i % 2 == 1)
        def _():
            fn(remote(sum2.at[slot, 1 - zl], rs3.at[i], qs.at[2, i], qr.at[2, i], to_z))

        @pl.when(i % 2 == 0)
        def _():
            fn(remote(sum2.at[slot, 1 - y], rs3.at[i], qs.at[2, i], qr.at[2, i], to_y))

    def got(copy):
        copy.wait_recv()

    def sent(copy):
        copy.wait_send()

    def drain_weights(*ms):
        for m in ms:
            if m >= 2:
                z_bulk(m, sent, every)
            if m >= 3:

                @pl.when(middle)
                def _():
                    each_share(m, lambda share: across(m, share).wait_send())

        def passed(owner):
            for m in ms:
                each_share(m, lambda share: x_copy(m, owner, share).wait_send())

        others(passed)

    def drain_early():
        drain_weights(0, 1, 2, 3, 4)

        @pl.when(f < 3)
        def _():
            for m in (0, 1):
                line_copy(m, f, f + 1, 4, True).wait_send()

        @pl.when(f > 0)
        def _():
            for m in (0, 1):
                line_copy(m, f, f - 1, 5, True).wait_send()

        for d in (1, 2, 3):
            for sign in (-1, 1):
                owner = f + sign * d
                after = f - sign

                @pl.when((owner >= 0) & (owner <= 3) & (after >= 0) & (after <= 3))
                def _():
                    for m in (0, 1):
                        line_copy(m, owner, after, owner, False).wait_send()

        def drain_chunks(j, carry):
            head_send(0, j, t, to_sib).wait_send()
            head_send(1, j, t, to_y).wait_send()
            head_send(2, j, ynb, to_sib).wait_send()
            hid_send(0, j, zl, t, to_sib).wait_send()
            hid_send(1, j, zl, t, to_y).wait_send()
            hid_send(2, j, zl, t, to_z).wait_send()
            hid_send(3, j, zl, ynb, to_sib).wait_send()
            hid_send(4, j, 1 - zl, t, to_sib).wait_send()
            hid_send(5, j, 1 - zl, t, to_y).wait_send()
            hid_send(6, j, 1 - zl, ynb, to_sib).wait_send()
            return carry

        lax.fori_loop(0, 4, drain_chunks, 0)

    def out_cols(n):
        owner, flip, half = place(n)
        return pl.ds(pl.multiple_of(owner * 2 * feat + half * feat, feat), feat)

    def out_copy(n):
        cols = out_cols(n)
        return pltpu.make_async_copy(outv.at[:, cols], out.at[0, :, cols], osem.at[n])

    def turn(i, carry):
        pl.when(i == 6)(drain_early)

        @pl.when((i == 1) & jnp.logical_not(middle))
        def _():
            pass_down(1)

        @pl.when(i == 3)
        def _():
            pass_down(2)

        @pl.when(i < blocks)
        def _():
            owner, flip, half = place(i)

            @pl.when((owner != f) & (flip == 1))
            def _():
                each_share(5, lambda share: x_arrived(5, owner, share))

            @pl.when(i >= 3)
            def _():
                q1(i - 3).wait_send()

            at = pl.ds(pl.multiple_of(owner * 2 * feat + half * feat, feat), feat)

            def down(cc, units):
                return lax.dot_general(
                    prod[pl.ds(pl.multiple_of(cc * 4 * chunk, chunk), 4 * chunk), :units],
                    wd[at, :units],
                    (((1,), (1,)), ((), ())),
                    preferred_element_type=F32,
                ).astype(BF16)

            def down_rows(cc):
                @pl.when(middle)
                def _():
                    part[i % 3, cc] = down(cc, 2 * hw)

                @pl.when(jnp.logical_not(middle))
                def _():
                    part[i % 3, cc] = down(cc, hw)

            down_rows(1 - c)
            q1(i).start()
            down_rows(c)

        @pl.when((i >= 1) & (i <= blocks))
        def _():
            n = i - 1
            q1(n).wait_recv()

            total = (part[n % 3, c].astype(F32) + rs1[n].astype(F32)).astype(BF16)
            sum1[n] = total.reshape(2, 2, chunk, feat)
            q2(n, start)

        @pl.when((i >= 3) & (i <= blocks + 2))
        def _():
            n = i - 3
            q2(n, got)


            @pl.when(n % 2 == 1)
            def _():
                sum2[n] = (sum1[n, y].astype(F32) + rs2[n].astype(F32)).astype(BF16)

            @pl.when(n % 2 == 0)
            def _():
                sum2[n] = (sum1[n, :, zl].astype(F32) + rs2[n].astype(F32)).astype(BF16)

            q3(n, start)

        @pl.when(i >= 5)
        def _():
            n = i - 5
            q3(n, got)
            mine = jnp.where(n % 2 == 1, zl, y)
            cols = out_cols(n)
            base = hid[zl, pl.ds(pl.multiple_of(t * chunk, chunk), chunk), cols].astype(F32)
            total = base + (sum2[n, mine].astype(F32) + rs3[n].astype(F32))
            outv[:, cols] = total.astype(BF16)
            out_copy(n).start()

        return carry

    with jax.named_scope("rs"):
        lax.fori_loop(0, blocks + 5, turn, 0)

    for n in range(blocks):
        if n >= blocks - 3:
            q1(n).wait_send()
        q2(n, sent)
        q3(n, sent)

    with jax.named_scope("drain"):
        drain_weights(5)
        for n in range(blocks):
            out_copy(n).wait()


def fused(*arrays):
    (tokens, mix_gain, value_w, gate_w, mix_taps, head_gain, out_w, ffn_gain, ffgate_w, up_w, ff_taps, down_w) = arrays
    _, length, width = tokens.shape
    fs = lax.axis_size("fs")
    cw, ow = value_w.shape[1], out_w.shape[1]
    hw = ffgate_w.shape[1] // 3
    chunk = length // 4
    feat = down_w.shape[0] // 2
    scratch = [
        pltpu.VMEM((length, width), BF16),
        pltpu.VMEM((length, width), BF16),
        pltpu.VMEM((fs * value_w.shape[0], 2 * cw), BF16),
        pltpu.VMEM((fs * out_w.shape[0], ow), BF16),
        pltpu.VMEM((length + 40, cw), F32),
        pltpu.VMEM((length, 4 * cw), BF16),
        pltpu.VMEM((2, length, width), BF16),
        pltpu.VMEM((8 * mix_taps.shape[0], cw), F32),
        pltpu.VMEM((2, fs * ffgate_w.shape[0], hw), BF16),
        pltpu.VMEM((2, fs * up_w.shape[0], hw), BF16),
        pltpu.VMEM((fs * down_w.shape[0], 2 * hw), BF16),
        pltpu.VMEM((chunk + 8, hw), F32),
        pltpu.VMEM((2 * length, 2 * hw), BF16),
        pltpu.VMEM((3, 2, 4 * chunk, feat), BF16),
        pltpu.VMEM((8, 4 * chunk, feat), BF16),
        pltpu.VMEM((8, 2, 2, chunk, feat), BF16),
        pltpu.VMEM((8, 2, chunk, feat), BF16),
        pltpu.VMEM((8, 2, chunk, feat), BF16),
        pltpu.VMEM((8, chunk, feat), BF16),
        pltpu.VMEM((chunk, width), BF16),
        pltpu.SemaphoreType.DMA((8,)),
        pltpu.SemaphoreType.DMA((6, 2)),
        pltpu.SemaphoreType.DMA((4,)),
    ]
    scratch += [pltpu.SemaphoreType.DMA((6, n, 2)) for n in (6, 4, 4, 4)]
    scratch += [pltpu.SemaphoreType.DMA((3, 4))] * 2
    scratch += [pltpu.SemaphoreType.DMA((7, 4))] * 2
    scratch += [pltpu.SemaphoreType.DMA((3, 8))] * 2
    anywhere = pl.BlockSpec(memory_space=pl.ANY)
    small = pl.BlockSpec(memory_space=pltpu.VMEM)
    return pl.pallas_call(
        kernel,
        out_shape=jax.ShapeDtypeStruct((1, chunk, width), BF16),
        in_specs=[anywhere, small, anywhere, anywhere, small, small, anywhere, small, anywhere, anywhere, small, anywhere],
        out_specs=anywhere,
        scratch_shapes=scratch,
        compiler_params=pltpu.CompilerParams(
            collective_id=0, has_side_effects=True, vmem_limit_bytes=67043328
        ),
        name="layer",
    )(
        tokens,
        mix_gain,
        value_w,
        gate_w,
        mix_taps,
        head_gain,
        out_w,
        ffn_gain,
        ffgate_w,
        up_w,
        ff_taps,
        down_w,
    )


def solution(mesh):
    placed = (
        P(("rep", "fs"), None, None),
        P(),
        P("fs", "tp"),
        P("fs", "tp"),
        P(None, "tp"),
        P("tp"),
        P("fs", "tp"),
        P(),
        P("fs", "tp"),
        P("fs", "tp"),
        P(None, "tp"),
        P("fs", "tp"),
    )
    shape = mesh.shape
    small = shape["rep"] == 2 and shape["fs"] == 4 and shape["tp"] == 4
    return jax.shard_map(
        fused if small else plain,
        mesh=mesh,
        in_specs=placed,
        out_specs=P(("rep", "fs"), "tp", None),
        check_vma=False,
    )
```

```python
import functools

import jax
import jax.numpy as jnp
from jax import lax
from jax.experimental import pallas as pl
from jax.experimental.pallas import tpu as pltpu
from jax.sharding import PartitionSpec as P

HEAD = 128
MESH = pl.DeviceIdType.MESH
F32 = jnp.float32
BF16 = jnp.bfloat16
norm_floor = 0.01


def row_norm(floats_in, scales):
    floats = floats_in.astype(F32)
    scaled = floats * lax.rsqrt(jnp.mean(floats * floats, axis=-1, keepdims=True) + norm_floor)
    return (scaled * scales.astype(F32)).astype(BF16)


def causal_conv(signal, kernel_taps):
    reach = kernel_taps.shape[0]
    length = signal.shape[0]
    padded = jnp.pad(signal, ((reach - 1, 0), (0, 0)))
    summed = padded[0:length] * kernel_taps[0]
    for offset in range(1, reach):
        summed = summed + padded[offset : offset + length] * kernel_taps[offset]
    return summed


def head_norm(signal, scales):
    heads = []
    for start in range(0, signal.shape[1], HEAD):
        part = signal[:, start : start + HEAD]
        centre = part - jnp.mean(part, axis=-1, keepdims=True)
        spread = jnp.mean(centre * centre, axis=-1, keepdims=True)
        gain = scales[start : start + HEAD].astype(F32)
        heads.append(jax.nn.silu(centre * lax.rsqrt(spread + norm_floor) * gain))
    return jnp.concatenate(heads, axis=1).astype(BF16)


def plain(
    tokens,
    mix_gain,
    value_weight,
    gate_weight,
    mix_taps,
    head_gain,
    out_weight,
    ffn_gain,
    ffgate_weight,
    up_weight,
    ff_taps,
    down_weight,
):
    def rows_of(shard):
        return lax.all_gather(shard, "fs", axis=0, tiled=True)

    sequence = tokens[0]
    width = value_weight.shape[1]
    pair_full = rows_of(jnp.concatenate([value_weight, gate_weight], axis=1))
    out_full = rows_of(out_weight)
    normed = row_norm(sequence, mix_gain)
    both = jnp.dot(normed, pair_full, preferred_element_type=F32)
    glu_out = both[:, :width] * jax.nn.sigmoid(both[:, width:])
    mixed_pos = causal_conv(glu_out, mix_taps.astype(F32))
    head_out = head_norm(mixed_pos, head_gain)
    out_cols = out_full.shape[1]
    all_heads = lax.all_gather(head_out, "tp", axis=1, tiled=True)
    own_cols = lax.dynamic_slice_in_dim(sequence, lax.axis_index("tp") * out_cols, out_cols, 1)
    mixer_sum = jnp.dot(all_heads, out_full, preferred_element_type=F32)
    hidden_cols = (own_cols.astype(F32) + mixer_sum).astype(BF16)
    full_rows = lax.all_gather(hidden_cols, "tp", axis=1, tiled=True)
    normed_ffn = row_norm(full_rows, ffn_gain)
    ffgate = jnp.dot(normed_ffn, rows_of(ffgate_weight), preferred_element_type=F32)
    gated = jax.nn.silu(causal_conv(ffgate, ff_taps.astype(F32)))
    ff_up = jnp.dot(normed_ffn, rows_of(up_weight), preferred_element_type=F32)
    product = (gated * ff_up).astype(BF16)
    own_count = sequence.shape[0] // lax.axis_size("tp")
    own_rows = lax.dynamic_slice_in_dim(full_rows, lax.axis_index("tp") * own_count, own_count, 0)
    partial = lax.dot_general(
        product, rows_of(down_weight), (((1,), (1,)), ((), ())), preferred_element_type=F32
    )
    result = lax.psum_scatter(partial.astype(BF16), "tp", scatter_dimension=0, tiled=True)
    return (own_rows.astype(F32) + result.astype(F32)).astype(BF16)[None]


def kernel(
    tokens,
    mix_gain,
    value_w,
    gate_w,
    mix_taps,
    head_gain,
    out_w,
    ffn_gain,
    ffgate_w,
    up_w,
    ff_taps,
    down_w,
    out,
    tok,
    normed,
    wpair,
    wout,
    glu,
    heads,
    hid,
    tapb,
    wg,
    wu,
    wd,
    gbuf,
    prod,
    part,
    rs1,
    sum1,
    rs2,
    sum2,
    rs3,
    outv,
    osem,
    loc,
    tsem,
    zs,
    zr,
    xs,
    xr,
    hs,
    hr,
    es,
    er,
    qs,
    qr,
):
    r, f, t = lax.axis_index("rep"), lax.axis_index("fs"), lax.axis_index("tp")
    y, c = t // 2, t % 2
    zl, zh = f % 2, f // 2
    fp = f + 1 - 2 * zl
    sib, ynb = t + 1 - 2 * c, (t + 2) % 4
    far = (sib + 2) % 4
    to_x, to_z, to_sib, to_y = {"rep": 1 - r}, {"fs": fp}, {"tp": sib}, {"tp": ynb}

    length, width = tok.shape
    chunk = length // 4
    cw = value_w.shape[1]
    ow = out_w.shape[1]
    hw = wg.shape[2]
    feat = down_w.shape[0] // 2

    def remote(src, dst, ss, rs, where):
        return pltpu.make_async_remote_copy(
            src_ref=src, dst_ref=dst, send_sem=ss, recv_sem=rs, device_id=where, device_id_type=MESH
        )

    barrier = pltpu.get_barrier_semaphore()
    for peer in (to_x, to_sib, to_y, {"fs": (f + 1) % 4}, {"fs": (f + 2) % 4}, {"fs": (f + 3) % 4}):
        pl.semaphore_signal(barrier, inc=1, device_id=peer, device_id_type=MESH)

    def rows(j):
        return pl.ds(pl.multiple_of(j * chunk, chunk), chunk)

    def tok_copy(j):
        return pltpu.make_async_copy(tokens.at[0, rows(j), :], tok.at[rows(j), :], tsem.at[j])

    for j in range(4):
        tok_copy(j).start()

    middle = (f == 1) | (f == 2)
    shares = jnp.where(middle, 2, 1)
    mats = (
        (value_w, wpair, 0, False),
        (gate_w, wpair, cw, False),
        (out_w, wout, 0, False),
        (ffgate_w, wg, 0, True),
        (up_w, wu, 0, True),
        (down_w, wd, None, True),
    )

    def is_middle(plane):
        return (plane == 1) | (plane == 2)

    def src_of(m, row, count, plane, share):
        w, dst, col, cut = mats[m]
        if cut:
            part_of = jnp.where(is_middle(plane), 1 + share, 0)
            return w.at[pl.ds(row, count), pl.ds(pl.multiple_of(part_of * hw, 128), hw)]
        return w.at[pl.ds(row, count), :]

    def dst_of(m, row, count, share):
        w, dst, col, cut = mats[m]
        if cut and col is None:
            return dst.at[pl.ds(row, count), pl.ds(share * hw, hw)]
        if cut:
            return dst.at[share, pl.ds(row, count), :]
        return dst.at[pl.ds(row, count), pl.ds(col, w.shape[1])]

    def piece(m, owner, half, share=0):
        n = mats[m][0].shape[0]
        return dst_of(m, pl.multiple_of(owner * n + half * (n // 2), n // 2), n // 2, share)

    def each_share(m, fn, plane=None):
        fn(0)
        if mats[m][3]:
            two = middle if plane is None else is_middle(plane)

            @pl.when(two)
            def _():
                fn(1)

    def own_copy(m, share):
        n = mats[m][0].shape[0]
        return pltpu.make_async_copy(
            src_of(m, 0, n, f, share), dst_of(m, pl.multiple_of(f * n, n), n, share), loc.at[m, share]
        )

    def z_copy(m, target, share):
        n = mats[m][0].shape[0]
        return remote(
            src_of(m, pl.multiple_of(r * (n // 2), n // 2), n // 2, target, share),
            piece(m, f, r, share),
            zs.at[m, target, share],
            zr.at[m, f, share],
            {"fs": target},
        )

    def z_arrived(m, owner, share=0):
        block = piece(m, owner, r, share)
        remote(block, block, zs.at[m, owner, share], zr.at[m, owner, share], to_x).wait_recv()

    def x_copy(m, owner, share=0):
        block = piece(m, owner, r, share)
        return remote(block, block, xs.at[m, owner, share], xr.at[m, owner, share], to_x)

    def x_arrived(m, owner, share=0):
        block = piece(m, owner, 1 - r, share)
        remote(block, block, xs.at[m, owner, share], xr.at[m, owner, share], to_x).wait_recv()

    def others(fn):
        def step(k, carry):
            fn(jnp.where(k == 0, fp, jnp.where(k == 1, 2 - zh, 3 - 3 * zh)))
            return carry

        lax.fori_loop(0, 3, step, 0)

    order = (fp, 2 - zh, 3 - 3 * zh)

    def line_copy(m, owner, target, slot, own):
        n = mats[m][0].shape[0]
        if own:
            src = src_of(m, pl.multiple_of(r * (n // 2), n // 2), n // 2, target, 0)
        else:
            src = piece(m, owner, r)
        return remote(src, piece(m, owner, r), zs.at[m, slot, 0], zr.at[m, owner, 0], {"fs": target})

    def z_bulk(m, fn, keep, shares_of=(0, 1)):
        def one(target):
            ok = keep(target)
            if mats[m][3]:
                ok = ok & (middle | (target != order[1]))

            for share in shares_of:
                if share == 1 and not mats[m][3]:
                    continue
                has = ok & is_middle(target) if share == 1 else ok

                @pl.when(has)
                def _():
                    fn(z_copy(m, target, share))

        others(one)

    def across(m, share):
        block = piece(m, fp, r, share)
        return remote(block, block, zs.at[m, f, share], zr.at[m, fp, share], {"fs": 3 - f})

    for m in range(6):
        each_share(m, lambda share: own_copy(m, share).start())
    with jax.named_scope("barrier"):
        pl.semaphore_wait(barrier, 6)

    def start(copy):
        copy.start()

    def every(target):
        return target >= 0

    def ends_only(target):
        return jnp.logical_not(is_middle(target))

    def pass_on(m, k, share):
        owner = order[k]
        z_arrived(m, owner, share)
        if mats[m][3] and k == 0:

            @pl.when(middle)
            def _():
                across(m, share).start()

        x_copy(m, owner, share).start()

    def relay(d):
        for sign in (-1, 1):
            owner = f + sign * d

            @pl.when((owner >= 0) & (owner <= 3))
            def _():
                for m in (0, 1):
                    z_arrived(m, owner)
                    after = f - sign

                    @pl.when((after >= 0) & (after <= 3))
                    def _():
                        line_copy(m, owner, after, owner, False).start()

                    x_copy(m, owner).start()


    def collect(share, *ms):
        def one(owner):
            for m in ms:
                x_arrived(m, owner, share)

        others(one)
        for m in ms:
            own_copy(m, share).wait()

    @pl.when(f < 3)
    def _():
        for m in (0, 1):
            line_copy(m, f, f + 1, 4, True).start()

    @pl.when(f > 0)
    def _():
        for m in (0, 1):
            line_copy(m, f, f - 1, 5, True).start()

    @pl.when(jnp.logical_not(middle))
    def _():
        for m in (3, 4):
            z_bulk(m, start, is_middle, (0,))

    def norm_rows(src, dst, gain_ref, count):
        gain = gain_ref[...].astype(F32).reshape(1, width)

        def step(i, carry):
            at = pl.ds(pl.multiple_of(i * 16, 16), 16)
            v = src[at, :].astype(F32)
            s = lax.rsqrt(jnp.mean(v * v, axis=-1, keepdims=True) + norm_floor)
            dst[at, :] = (v * s * gain).astype(BF16)
            return carry

        lax.fori_loop(0, count // 16, step, 0, unroll=4)

    glu[pl.ds(0, 32), :] = jnp.zeros((32, cw), F32)
    for k in range(mix_taps.shape[0]):
        tapb[pl.ds(8 * k, 8), :] = jnp.broadcast_to(mix_taps[k : k + 1, :].astype(F32), (8, mix_taps.shape[1]))
    with jax.named_scope("tokwait"):
        for j in range(4):
            tok_copy(j).wait()
        norm_rows(tok, normed, mix_gain, length)

    with jax.named_scope("pass01"):
        for d in (1, 2, 3):
            relay(d)
    @pl.when(middle)
    def _():
        for m in (3, 4):
            z_bulk(m, start, is_middle, (0,))

    with jax.named_scope("coll01"):
        collect(0, 0, 1)
    z_bulk(2, start, every)

    @pl.when(jnp.logical_not(middle))
    def _():
        for m in (3, 4):
            z_bulk(m, start, every, (1,))


    def head_cols(who):
        return pl.ds(pl.multiple_of(who * cw, 128), cw)

    def head_send(kind, j, who, where):
        block = heads.at[rows(j), head_cols(who)]
        return remote(block, block, hs.at[kind, j], hr.at[kind, j], where)

    def head_wait(kind, j, who):
        block = heads.at[rows(j), head_cols(who)]
        remote(block, block, hs.at[kind, j], hr.at[kind, j], to_sib).wait_recv()

    reach = mix_taps.shape[0]
    sub = 64

    hgain = head_gain[...].astype(F32).reshape(1, cw)

    def mix_chunk(j, carry):
        both = jnp.dot(normed[rows(j), :], wpair[...], preferred_element_type=F32)
        glu[pl.ds(pl.multiple_of(j * chunk + 32, 32), chunk), :] = both[:, :cw] * jax.nn.sigmoid(both[:, cw:])

        def conv_step(i, inner):
            base = pl.multiple_of(j * chunk + i * sub, sub)
            acc = None
            for e in range(8):
                rot = None
                for o in range(e, 33, 8):
                    k = o - (33 - reach)
                    if 0 <= k < reach:
                        view = glu[pl.ds(base + 8 * (o // 8), sub + 8), :].reshape(sub // 8 + 1, 8, cw)
                        term = view * tapb[pl.ds(8 * k, 8), :][None]
                        rot = term if rot is None else rot + term
                part_sum = rot.reshape(sub + 8, cw)[e : e + sub, :]
                acc = part_sum if acc is None else acc + part_sum
            parts = []
            for h in range(0, cw, HEAD):
                v = acc[:, h : h + HEAD]
                v = v - jnp.mean(v, axis=-1, keepdims=True)
                s = lax.rsqrt(jnp.mean(v * v, axis=-1, keepdims=True) + norm_floor)
                v = v * s * hgain[:, h : h + HEAD]
                parts.append(v * jax.nn.sigmoid(v))
            heads[pl.ds(base, sub), head_cols(t)] = jnp.concatenate(parts, axis=1).astype(BF16)
            return inner

        lax.fori_loop(0, chunk // sub, conv_step, 0)
        head_send(0, j, t, to_sib).start()
        head_send(1, j, t, to_y).start()
        return carry

    with jax.named_scope("mix"):
        lax.fori_loop(0, 4, mix_chunk, 0)
    with jax.named_scope("pass2"):
        for k in (0, 1, 2):
            pass_on(2, k, 0)

        @pl.when(middle)
        def _():
            for m in (3, 4):
                pass_on(m, 0, 0)

    @pl.when(middle)
    def _():
        for m in (3, 4):
            z_bulk(m, start, lambda target: target == fp, (0,))

    def heads_on(j, carry):
        head_wait(1, j, ynb)
        head_send(2, j, ynb, to_sib).start()
        return carry

    with jax.named_scope("heads_on"):
        lax.fori_loop(0, 4, heads_on, 0)
    with jax.named_scope("coll2"):
        collect(0, 2)

    def hid_block(seq, j, who):
        return hid.at[seq, rows(j), pl.ds(pl.multiple_of(who * ow, 128), ow)]

    def hid_send(kind, j, seq, who, where):
        block = hid_block(seq, j, who)
        return remote(block, block, es.at[kind, j], er.at[kind, j], where)

    def hid_wait(kind, j, seq, who):
        block = hid_block(seq, j, who)
        remote(block, block, es.at[kind, j], er.at[kind, j], to_sib).wait_recv()

    def out_chunk(j, carry):
        head_wait(0, j, sib)
        head_wait(2, j, far)
        own = tok[rows(j), pl.ds(pl.multiple_of(t * ow, 128), ow)].astype(F32)
        total = own + jnp.dot(heads[rows(j), :], wout[...], preferred_element_type=F32)
        hid[zl, rows(j), pl.ds(pl.multiple_of(t * ow, 128), ow)] = total.astype(BF16)
        hid_send(0, j, zl, t, to_sib).start()
        hid_send(1, j, zl, t, to_y).start()

        @pl.when(jnp.logical_not(middle))
        def _():
            hid_send(2, j, zl, t, to_z).start()

        return carry

    with jax.named_scope("outmm"):
        lax.fori_loop(0, 4, out_chunk, 0)

    for m in (3, 4):
        z_bulk(m, start, lambda target: ends_only(target) & (target != fp), (0,))

    @pl.when(middle)
    def _():
        for j in range(4):
            hid_send(2, j, zl, t, to_z).start()
        for m in (3, 4):
            z_bulk(m, start, every, (1,))

    @pl.when(jnp.logical_not(middle))
    def _():
        z_bulk(5, start, is_middle)

    with jax.named_scope("pass1"):

        @pl.when(middle)
        def _():
            for m in (3, 4):
                pass_on(m, 1, 0)

        @pl.when(jnp.logical_not(middle))
        def _():
            for m in (3, 4):
                pass_on(m, 0, 0)

    def hid_own(j, carry):
        hid_wait(1, j, zl, ynb)
        hid_send(3, j, zl, ynb, to_sib).start()

        @pl.when(middle & (j == 2))
        def _():
            for m in (3, 4):
                pass_on(m, 2, 0)

        return carry

    with jax.named_scope("hid_own"):
        lax.fori_loop(0, 4, hid_own, 0)

    with jax.named_scope("passE"):

        @pl.when(jnp.logical_not(middle))
        def _():
            for k in (1, 2):
                for m in (3, 4):
                    pass_on(m, k, 0)

    with jax.named_scope("pass0s1"):

        @pl.when(middle)
        def _():
            for m in (3, 4):
                pass_on(m, 0, 1)
            z_bulk(5, start, is_middle)

    def hid_partner(j, carry):
        hid_wait(2, j, 1 - zl, t)
        hid_send(4, j, 1 - zl, t, to_sib).start()
        hid_send(5, j, 1 - zl, t, to_y).start()
        return carry

    freach = ff_taps.shape[0]
    asub = 32

    def kept_rows(mine, j):
        return (normed if mine else tok)[rows(j), :]

    def prod_row(mine, j):
        seq = zl if mine else 1 - zl
        return pl.multiple_of((4 * (j % 2) + 2 * (j // 2) + seq) * chunk, chunk)

    def gate_rows(share, mine, j):
        if share == 0:
            kept = normed if mine else tok
            seq = zl if mine else 1 - zl
            norm_rows(hid.at[seq, rows(j), :], kept.at[rows(j), :], ffn_gain, chunk)
        part_of = jnp.where(middle, 1 + share, 0)
        ftap = ff_taps[:, pl.ds(pl.multiple_of(part_of * hw, 128), hw)].astype(F32)
        gbuf[pl.ds(0, 8), :] = gbuf[pl.ds(chunk, 8), :]

        @pl.when(j == 0)
        def _():
            gbuf[pl.ds(0, 8), :] = jnp.zeros((8, hw), F32)

        gbuf[pl.ds(8, chunk), :] = jnp.dot(kept_rows(mine, j), wg[share], preferred_element_type=F32)

        def act(a, inner):
            base = pl.multiple_of(a * asub, asub)
            window = gbuf[pl.ds(base, asub + 8), :]
            acc = None
            for k in range(freach):
                o = 8 - (freach - 1) + k
                term = window[o : o + asub, :] * ftap[k : k + 1, :]
                acc = term if acc is None else acc + term
            gated = (acc * jax.nn.sigmoid(acc)).astype(BF16)
            prod[pl.ds(prod_row(mine, j) + base, asub), share * hw : (share + 1) * hw] = gated
            return inner

        lax.fori_loop(0, chunk // asub, act, 0)

    def up_rows(share, mine, j):
        at = pl.ds(prod_row(mine, j), chunk)
        cols = slice(share * hw, (share + 1) * hw)
        ff_up = jnp.dot(kept_rows(mine, j), wu[share], preferred_element_type=F32)
        prod[at, cols] = (prod[at, cols].astype(F32) * ff_up).astype(BF16)

    def pass_down(k):
        each_share(5, lambda share: pass_on(5, k, share))

    def hid_last(j):
        hid_wait(5, j, 1 - zl, ynb)
        hid_send(6, j, 1 - zl, ynb, to_sib).start()

    def own_ready(j):
        hid_wait(0, j, zl, sib)
        hid_wait(3, j, zl, far)

    def partner_ready(j):
        hid_wait(4, j, 1 - zl, sib)
        hid_wait(6, j, 1 - zl, far)

    def four(fn):
        def step(j, carry):
            fn(j)
            return carry

        lax.fori_loop(0, 4, step, 0)

    @pl.when(middle)
    def _():
        with jax.named_scope("hid_partner"):
            lax.fori_loop(0, 4, hid_partner, 0)
        with jax.named_scope("collect"):
            collect(0, 3, 4)

        def own(j):
            own_ready(j)
            gate_rows(0, True, j)
            up_rows(0, True, j)
            pl.when(j >= 1)(lambda: hid_last(j - 1))

        def partner(j):
            pl.when(j == 0)(lambda: hid_last(3))
            partner_ready(j)
            gate_rows(0, False, j)
            up_rows(0, False, j)

        with jax.named_scope("ffn1"):
            four(own)
            for m in (3, 4):
                pass_on(m, 1, 1)
            z_bulk(5, start, ends_only, (0,))
            four(partner)
        with jax.named_scope("coll1g"):
            pass_on(3, 2, 1)
            collect(1, 3)

        def own_gate(j):
            gate_rows(1, True, j)
            pl.when(j == 0)(lambda: pass_on(4, 2, 1))

        with jax.named_scope("gate2"):
            four(own_gate)
            four(lambda j: gate_rows(1, False, j))
        with jax.named_scope("coll1u"):
            collect(1, 4)
        with jax.named_scope("up2"):
            pass_down(0)
            four(lambda j: up_rows(1, True, j))
            pass_down(1)
            four(lambda j: up_rows(1, False, j))

    @pl.when(jnp.logical_not(middle))
    def _():
        with jax.named_scope("hid_partner"):
            lax.fori_loop(0, 2, hid_partner, 0)
        with jax.named_scope("collect"):
            collect(0, 3)

        def own_gate(j):
            own_ready(j)
            gate_rows(0, True, j)
            pl.when(j < 2)(lambda: hid_partner(j + 2, None))
            pl.when(j == 2)(lambda: hid_last(0))

        with jax.named_scope("gate1"):
            four(own_gate)
        with jax.named_scope("coll0u"):
            collect(0, 4)
            z_bulk(5, start, ends_only, (0,))

        def partner(j):
            partner_ready(j)
            gate_rows(0, False, j)
            up_rows(0, False, j)
            pl.when(j == 0)(lambda: hid_last(3))
            pl.when(j == 2)(lambda: pass_down(0))

        with jax.named_scope("up1"):
            four(lambda j: up_rows(0, True, j))
            hid_last(1)
            hid_last(2)
        with jax.named_scope("ffnp"):
            four(partner)

    with jax.named_scope("own5"):
        each_share(5, lambda share: own_copy(5, share).wait())
    blocks = 8

    def place(i):
        late = i // 4
        k = i % 4
        flip = k // 2
        early_owner = jnp.where(k % 2 == 0, 3 * zh, 1 + zh)
        late_owner = jnp.where(k % 2 == 0, 2 - zh, 3 - 3 * zh)
        owner = jnp.where(late == 0, early_owner, late_owner)
        half = jnp.where(flip == 0, r, 1 - r)
        return owner, flip, half

    def q1(i):
        return remote(part.at[i % 3, 1 - c], rs1.at[i], qs.at[0, i], qr.at[0, i], to_sib)

    def q2(i, fn):
        slot = i

        @pl.when(i % 2 == 1)
        def _():
            fn(remote(sum1.at[slot, 1 - y], rs2.at[i], qs.at[1, i], qr.at[1, i], to_y))

        @pl.when(i % 2 == 0)
        def _():
            fn(remote(sum1.at[slot, :, 1 - zl], rs2.at[i], qs.at[1, i], qr.at[1, i], to_z))

    def q3(i, fn):
        slot = i

        @pl.when(i % 2 == 1)
        def _():
            fn(remote(sum2.at[slot, 1 - zl], rs3.at[i], qs.at[2, i], qr.at[2, i], to_z))

        @pl.when(i % 2 == 0)
        def _():
            fn(remote(sum2.at[slot, 1 - y], rs3.at[i], qs.at[2, i], qr.at[2, i], to_y))

    def got(copy):
        copy.wait_recv()

    def sent(copy):
        copy.wait_send()

    def drain_weights(*ms):
        for m in ms:
            if m >= 2:
                z_bulk(m, sent, every)
            if m >= 3:

                @pl.when(middle)
                def _():
                    each_share(m, lambda share: across(m, share).wait_send())

        def passed(owner):
            for m in ms:
                each_share(m, lambda share: x_copy(m, owner, share).wait_send())

        others(passed)

    def drain_early():
        drain_weights(0, 1, 2, 3, 4)

        @pl.when(f < 3)
        def _():
            for m in (0, 1):
                line_copy(m, f, f + 1, 4, True).wait_send()

        @pl.when(f > 0)
        def _():
            for m in (0, 1):
                line_copy(m, f, f - 1, 5, True).wait_send()

        for d in (1, 2, 3):
            for sign in (-1, 1):
                owner = f + sign * d
                after = f - sign

                @pl.when((owner >= 0) & (owner <= 3) & (after >= 0) & (after <= 3))
                def _():
                    for m in (0, 1):
                        line_copy(m, owner, after, owner, False).wait_send()

        def drain_chunks(j, carry):
            head_send(0, j, t, to_sib).wait_send()
            head_send(1, j, t, to_y).wait_send()
            head_send(2, j, ynb, to_sib).wait_send()
            hid_send(0, j, zl, t, to_sib).wait_send()
            hid_send(1, j, zl, t, to_y).wait_send()
            hid_send(2, j, zl, t, to_z).wait_send()
            hid_send(3, j, zl, ynb, to_sib).wait_send()
            hid_send(4, j, 1 - zl, t, to_sib).wait_send()
            hid_send(5, j, 1 - zl, t, to_y).wait_send()
            hid_send(6, j, 1 - zl, ynb, to_sib).wait_send()
            return carry

        lax.fori_loop(0, 4, drain_chunks, 0)

    def out_cols(n):
        owner, flip, half = place(n)
        return pl.ds(pl.multiple_of(owner * 2 * feat + half * feat, feat), feat)

    def out_copy(n):
        cols = out_cols(n)
        return pltpu.make_async_copy(outv.at[:, cols], out.at[0, :, cols], osem.at[n])

    def turn(i, carry):
        pl.when(i == 6)(drain_early)

        @pl.when((i == 1) & jnp.logical_not(middle))
        def _():
            pass_down(1)

        @pl.when(i == 3)
        def _():
            pass_down(2)

        @pl.when(i < blocks)
        def _():
            owner, flip, half = place(i)

            @pl.when((owner != f) & (flip == 1))
            def _():
                each_share(5, lambda share: x_arrived(5, owner, share))

            @pl.when(i >= 3)
            def _():
                q1(i - 3).wait_send()

            at = pl.ds(pl.multiple_of(owner * 2 * feat + half * feat, feat), feat)

            def down(cc, units):
                return lax.dot_general(
                    prod[pl.ds(pl.multiple_of(cc * 4 * chunk, chunk), 4 * chunk), :units],
                    wd[at, :units],
                    (((1,), (1,)), ((), ())),
                    preferred_element_type=F32,
                ).astype(BF16)

            def down_rows(cc):
                @pl.when(middle)
                def _():
                    part[i % 3, cc] = down(cc, 2 * hw)

                @pl.when(jnp.logical_not(middle))
                def _():
                    part[i % 3, cc] = down(cc, hw)

            down_rows(1 - c)
            q1(i).start()
            down_rows(c)

        @pl.when(i < blocks)
        def _():
            n = i
            q1(n).wait_recv()

            total = (part[n % 3, c].astype(F32) + rs1[n].astype(F32)).astype(BF16)
            sum1[n] = total.reshape(2, 2, chunk, feat)
            q2(n, start)

        @pl.when((i >= 2) & (i <= blocks + 1))
        def _():
            n = i - 2
            q2(n, got)


            @pl.when(n % 2 == 1)
            def _():
                sum2[n] = (sum1[n, y].astype(F32) + rs2[n].astype(F32)).astype(BF16)

            @pl.when(n % 2 == 0)
            def _():
                sum2[n] = (sum1[n, :, zl].astype(F32) + rs2[n].astype(F32)).astype(BF16)

            q3(n, start)

        @pl.when(i >= 4)
        def _():
            n = i - 4
            q3(n, got)
            mine = jnp.where(n % 2 == 1, zl, y)
            cols = out_cols(n)
            base = hid[zl, pl.ds(pl.multiple_of(t * chunk, chunk), chunk), cols].astype(F32)
            total = base + (sum2[n, mine].astype(F32) + rs3[n].astype(F32))
            outv[:, cols] = total.astype(BF16)
            out_copy(n).start()

        return carry

    with jax.named_scope("rs"):
        lax.fori_loop(0, blocks + 4, turn, 0)

    for n in range(blocks):
        if n >= blocks - 3:
            q1(n).wait_send()
        q2(n, sent)
        q3(n, sent)

    with jax.named_scope("drain"):
        drain_weights(5)
        for n in range(blocks):
            out_copy(n).wait()


def fused(*arrays):
    (tokens, mix_gain, value_w, gate_w, mix_taps, head_gain, out_w, ffn_gain, ffgate_w, up_w, ff_taps, down_w) = arrays
    _, length, width = tokens.shape
    fs = lax.axis_size("fs")
    cw, ow = value_w.shape[1], out_w.shape[1]
    hw = ffgate_w.shape[1] // 3
    chunk = length // 4
    feat = down_w.shape[0] // 2
    scratch = [
        pltpu.VMEM((length, width), BF16),
        pltpu.VMEM((length, width), BF16),
        pltpu.VMEM((fs * value_w.shape[0], 2 * cw), BF16),
        pltpu.VMEM((fs * out_w.shape[0], ow), BF16),
        pltpu.VMEM((length + 40, cw), F32),
        pltpu.VMEM((length, 4 * cw), BF16),
        pltpu.VMEM((2, length, width), BF16),
        pltpu.VMEM((8 * mix_taps.shape[0], cw), F32),
        pltpu.VMEM((2, fs * ffgate_w.shape[0], hw), BF16),
        pltpu.VMEM((2, fs * up_w.shape[0], hw), BF16),
        pltpu.VMEM((fs * down_w.shape[0], 2 * hw), BF16),
        pltpu.VMEM((chunk + 8, hw), F32),
        pltpu.VMEM((2 * length, 2 * hw), BF16),
        pltpu.VMEM((3, 2, 4 * chunk, feat), BF16),
        pltpu.VMEM((8, 4 * chunk, feat), BF16),
        pltpu.VMEM((8, 2, 2, chunk, feat), BF16),
        pltpu.VMEM((8, 2, chunk, feat), BF16),
        pltpu.VMEM((8, 2, chunk, feat), BF16),
        pltpu.VMEM((8, chunk, feat), BF16),
        pltpu.VMEM((chunk, width), BF16),
        pltpu.SemaphoreType.DMA((8,)),
        pltpu.SemaphoreType.DMA((6, 2)),
        pltpu.SemaphoreType.DMA((4,)),
    ]
    scratch += [pltpu.SemaphoreType.DMA((6, n, 2)) for n in (6, 4, 4, 4)]
    scratch += [pltpu.SemaphoreType.DMA((3, 4))] * 2
    scratch += [pltpu.SemaphoreType.DMA((7, 4))] * 2
    scratch += [pltpu.SemaphoreType.DMA((3, 8))] * 2
    anywhere = pl.BlockSpec(memory_space=pl.ANY)
    small = pl.BlockSpec(memory_space=pltpu.VMEM)
    return pl.pallas_call(
        kernel,
        out_shape=jax.ShapeDtypeStruct((1, chunk, width), BF16),
        in_specs=[anywhere, small, anywhere, anywhere, small, small, anywhere, small, anywhere, anywhere, small, anywhere],
        out_specs=anywhere,
        scratch_shapes=scratch,
        compiler_params=pltpu.CompilerParams(
            collective_id=0, has_side_effects=True, vmem_limit_bytes=67043328
        ),
        name="layer",
    )(
        tokens,
        mix_gain,
        value_w,
        gate_w,
        mix_taps,
        head_gain,
        out_w,
        ffn_gain,
        ffgate_w,
        up_w,
        ff_taps,
        down_w,
    )


def solution(mesh):
    placed = (
        P(("rep", "fs"), None, None),
        P(),
        P("fs", "tp"),
        P("fs", "tp"),
        P(None, "tp"),
        P("tp"),
        P("fs", "tp"),
        P(),
        P("fs", "tp"),
        P("fs", "tp"),
        P(None, "tp"),
        P("fs", "tp"),
    )
    shape = mesh.shape
    small = shape["rep"] == 2 and shape["fs"] == 4 and shape["tp"] == 4
    return jax.shard_map(
        fused if small else plain,
        mesh=mesh,
        in_specs=placed,
        out_specs=P(("rep", "fs"), "tp", None),
        check_vma=False,
    )
```
